256 devices in a mesh: fs: 32 (over z, x), tp: 8 (over y, core).
Axes of the slice: x: 4, y: 4, z: 8, core: 2. Of those that a mesh axis runs over, the one named last changes fastest.
Arguments:
- tokens: bfloat16 [32768, 2048], P('fs', 'tp'), may hold values from -6 to 6
- grad_out: bfloat16 [32768, 2048], P('fs', 'tp'), may hold values from -6 to 6
- norm_gain: float32 [2048], replicated, may hold values from 0.1 to 1.9
- gate_weight: bfloat16 [3072, 2048], P('tp', 'fs'), may hold values from -0.125 to 0.125
- up_weight: bfloat16 [3072, 2048], P('tp', 'fs'), may hold values from -0.125 to 0.125
- down_weight: bfloat16 [3072, 2048], P('tp', 'fs'), may hold values from -0.109375 to 0.109375
Outputs:
- grad_input: bfloat16 [32768, 2048], P('fs', 'tp')
- grad_gate: float32 [3072, 2048], P('tp', 'fs')
- grad_up: float32 [3072, 2048], P('tp', 'fs')
- grad_down: float32 [3072, 2048], P('tp', 'fs')
- row_squares: float32 [3, 3072], P(None, 'tp')
The draws below stay inside these ranges and needn't reach their ends.
All inputs are finite; a program needn't handle non-finite values.
Results may differ from the reference program's by a relative error of at most 0.015.
Values may be sent and summed in bfloat16 or wider, within the bound.
A program may use at most 64 MiB of HBM per device.

```python
import jax
import jax.numpy as jnp
from jax import lax

D = 2048
FF = 3072
TOKENS = 32768
N_TP = 8


def with_spikes(drawn, rng, source, target, blocks, factor):
    owner, partner = [(jnp.arange(drawn.shape[dim]) // (drawn.shape[dim] // blocks)).reshape([-1 if axis == dim else 1 for axis in range(drawn.ndim)]) for dim in (source, target)]
    chosen = jax.random.permutation(rng, blocks)[partner]
    strong = (owner == chosen) | (owner == (partner + blocks // 2) % blocks)
    return jnp.where(strong, factor * drawn, drawn)


def levels(own_key, dims, split, least, top_value):
    level, own = 1.0, jax.random.fold_in(own_key, 6)
    for position, shards_of in split:
        heights = jnp.exp(jax.random.uniform(jax.random.fold_in(own, position), (shards_of,), jnp.float32, least / len(split), top_value / len(split)))
        level = level * jnp.repeat(heights, dims[position] // shards_of).reshape([-1 if axis == position else 1 for axis in range(len(dims))])
    return level


def noise(stream_key, dims, scale, reach, pieces=(), dtype=jnp.bfloat16):
    loudness = levels(stream_key, dims, pieces, -0.22, 0.18) if pieces else 1.0
    entries = jax.random.normal(stream_key, dims, jnp.float32) * scale * loudness
    return jnp.minimum(jnp.maximum(entries, -reach), reach).astype(dtype)


def bell_draw_with(stream_key, extent, spread, bound, split, heavy, dtype=jnp.bfloat16):
    entries = spread * jax.random.normal(stream_key, extent, jnp.float32)
    if split:
        entries = entries * levels(stream_key, extent, split, -0.22, 0.18)
    return jnp.clip(with_spikes(entries, jax.random.fold_in(stream_key, 3), *heavy), -bound, bound).astype(dtype)


def setup_inputs(seed: int = 0) -> dict:
    key_list = jax.random.split(jax.random.key(seed), 7)
    tokens = noise(key_list[0], (TOKENS, D), 1.0, 6.0, ((0, 32), (1, 8)))
    grad_out = bell_draw_with(key_list[1], (TOKENS, D), 1.0, 6.0, ((0, 32), (1, 8)), (0, 1, 32, 2.75))
    norm_gain = jnp.clip(1.0 + 0.18 * jax.random.normal(key_list[2], (D,), jnp.float32), 0.1, 1.9)
    gate_weight = noise(key_list[3], (FF, D), D ** -0.5, 0.125, ((0, 8), (1, 32)))
    up_weight = noise(key_list[4], (FF, D), D ** -0.5, 0.125, ((0, 8), (1, 32)))
    down_weight = noise(key_list[5], (FF, D), FF ** -0.5, 0.109375, ((0, 8), (1, 32)))
    return {"tokens": tokens, "grad_out": grad_out, "norm_gain": norm_gain, "gate_weight": gate_weight, "up_weight": up_weight, "down_weight": down_weight}


def rms_back(grad_rows, unit_rows, inv_rms, gain_rows):
    scaled = gain_rows * grad_rows
    inner = lax.optimization_barrier(jnp.mean(scaled * unit_rows, axis=-1, keepdims=True))
    return inv_rms * (scaled - unit_rows * inner)

def reference(tokens, grad_out, norm_gain, gate_weight, up_weight, down_weight):
    floated = tokens.astype(jnp.float32)
    inv_rms = lax.rsqrt(lax.optimization_barrier(jnp.mean(floated * floated, axis=-1, keepdims=True)) + 1e-06)
    unit_rows = floated * inv_rms
    gain_rows = norm_gain.astype(jnp.float32)[None, :]
    normed = (unit_rows * gain_rows).astype(jnp.bfloat16)
    gate_pre = jnp.dot(normed, gate_weight.T, preferred_element_type=jnp.float32)
    up_pre = jnp.dot(normed, up_weight.T, preferred_element_type=jnp.float32)
    sigma = jax.nn.sigmoid(gate_pre)
    active = gate_pre * sigma
    hidden = (active * up_pre).astype(jnp.bfloat16)
    grad_hidden = 0.5 * jnp.dot(grad_out, down_weight.T, preferred_element_type=jnp.float32)
    gate_grad_pre = (grad_hidden * up_pre * sigma * (1.0 + gate_pre * (1.0 - sigma))).astype(jnp.bfloat16)
    up_grad_pre = (grad_hidden * active).astype(jnp.bfloat16)
    factor = TOKENS ** (-0.5)
    grad_down = 0.5 * factor * jnp.dot(hidden.T, grad_out, preferred_element_type=jnp.float32)
    grad_gate = factor * jnp.dot(gate_grad_pre.T, normed, preferred_element_type=jnp.float32)
    grad_up = factor * jnp.dot(up_grad_pre.T, normed, preferred_element_type=jnp.float32)
    width = FF // N_TP
    total = jnp.zeros(tokens.shape, jnp.float32)
    for block in range(N_TP):
        lower = block * width
        upper = lower + width
        grad_rows = jnp.dot(gate_grad_pre[:, lower:upper], gate_weight[lower:upper], preferred_element_type=jnp.float32)
        grad_rows = grad_rows + jnp.dot(up_grad_pre[:, lower:upper], up_weight[lower:upper], preferred_element_type=jnp.float32)
        partial_k = rms_back(grad_rows, unit_rows, inv_rms, gain_rows).astype(jnp.bfloat16)
        total = total + partial_k.astype(jnp.float32)
    grad_input = (grad_out.astype(jnp.float32) + total).astype(jnp.bfloat16)
    row_squares = jnp.stack([lax.optimization_barrier(jnp.sum(grad_gate * grad_gate, axis=1)), lax.optimization_barrier(jnp.sum(grad_up * grad_up, axis=1)), lax.optimization_barrier(jnp.sum(grad_down * grad_down, axis=1))]) / D
    return (grad_input, grad_gate, grad_up, grad_down, row_squares)
```

```python
import jax
import jax.numpy as jnp
from jax import lax
from jax.experimental import pallas as pl
from jax.experimental.pallas import tpu as pltpu
from jax.sharding import Mesh
from jax.sharding import PartitionSpec as P

FS = ("z", "x")
TP = ("y", "c")
NZ, NX, NY, NC = 8, 4, 4, 2
F32, BF16 = jnp.float32, jnp.bfloat16
CHUNKS = 4
COPIES = 184
ORDER = (4, 3, -3, 2, -2, 1, -1, 0)


class Net:
    def __init__(self, send_sems, recv_sems):
        self.send_sems, self.recv_sems, self.copies = send_sems, recv_sems, []

    def send(self, src, dst, **to):
        at = len(self.copies)
        copy = pltpu.make_async_remote_copy(
            src_ref=src,
            dst_ref=dst,
            send_sem=self.send_sems.at[at],
            recv_sem=self.recv_sems.at[at],
            device_id=to,
            device_id_type=pl.DeviceIdType.MESH,
        )
        copy.start()
        self.copies.append(copy)
        return copy

    def finish(self):
        for copy in self.copies:
            copy.wait_send()


def lanes_summed(v):
    total = v[:, 0:128]
    for at in range(128, v.shape[1], 128):
        total = total + v[:, at : at + 128]
    return total


def turned(left, right):
    return lax.dot_general(left, right, (((0,), (0,)), ((), ())), preferred_element_type=F32)


def kernel(
    tok, grd, gain, wgu, wdn,
    out_in, out_gu, out_dn, out_sq,
    T, G, N, GU, DN, AB, H, INV, V, DGU, DDN,
    SX1, RX1, SX2, RX2, XR, SZ, RZ, SD, RD, FD, SE1, RE1, SE2, RE2,
    PP, PR, S1, R1, S2, R2, QX, QZ,
    send_sems, recv_sems, local_sems,
):
    z, x, y, c = (lax.axis_index(a) for a in ("z", "x", "y", "c"))
    zz = lambda d: lax.rem(z + (d + NZ), NZ)
    xx = lambda d: lax.rem(x + (d + NX), NX)
    yy = lambda d: lax.rem(y + (d + NY), NY)
    other = 1 - c
    me = y * NC + c
    slot = lambda d: yy(d) * NC + c
    tokens = tok.shape[0]
    rows = tokens // CHUNKS
    wide = tok.shape[1]
    ff = wdn.shape[1]
    model = wide * NY * NC
    part = wgu.shape[0]
    half_part, half_rows = part // 2, rows // 2
    gate, up = pl.ds(0, ff), pl.ds(ff, ff)
    factor = (tokens * NZ * NX) ** (-0.5)
    span = lambda ch: pl.ds(ch * rows, rows)

    barrier = pltpu.get_barrier_semaphore()
    peers = [{"z": zz(d)} for d in range(1, NZ)] + [{"x": xx(d)} for d in range(1, NX)]
    peers += [{"y": yy(1)}, {"y": yy(-1)}, {"c": other}]
    for peer in peers:
        pl.semaphore_signal(barrier, inc=1, device_id=peer, device_id_type=pl.DeviceIdType.MESH)
    locals_ = [
        pltpu.make_async_copy(src, dst, local_sems.at[i])
        for i, (src, dst) in enumerate(
            ((wgu, GU.at[z, x]), (wdn, DN.at[z, x]), (tok, T.at[me]), (grd, G.at[me]))
        )
    ]
    for copy in locals_:
        copy.start()
    pl.semaphore_wait(barrier, len(peers))
    net = Net(send_sems, recv_sems)

    gz, gx, gxf, dx, dxf, dz, ya, yb, dd = {}, {}, {}, {}, {}, {}, {}, {}, {}

    def gx_send(d, src):
        gx[d, 1] = net.send(src, GU.at[zz(d), x], x=xx(1))
        gx[d, -1] = net.send(src, GU.at[zz(d), x], x=xx(-1))

    def gx_pass(d):
        gx[d, 1].wait_recv()
        ref = GU.at[zz(d), xx(-1), :, gate]
        gxf[d, 1] = net.send(ref, ref, x=xx(1))
        gx[d, -1].wait_recv()
        ref = GU.at[zz(d), xx(1), :, up]
        gxf[d, -1] = net.send(ref, ref, x=xx(-1))

    def gz_step(s):
        for way in (1, -1):
            gz[s, way].wait_recv()
            if s < NZ // 2:
                ref = GU.at[zz(-way * s), x]
                if s == NZ // 2 - 1:
                    ref = GU.at[zz(-way * s), x, :, gate if way == 1 else up]
                gz[s + 1, way] = net.send(ref, ref, z=zz(way))
        if s < NZ // 2:
            gx_send(-s, GU.at[zz(-s), x])
            gx_send(s, GU.at[zz(s), x])
        else:
            gx_send(s, GU.at[zz(s), x])

    def dx_pass():
        dx[1].wait_recv()
        ref = DN.at[z, xx(-1), pl.ds(0, half_part)]
        dxf[1] = net.send(ref, ref, x=xx(1))
        dx[-1].wait_recv()
        ref = DN.at[z, xx(1), pl.ds(half_part, half_part)]
        dxf[-1] = net.send(ref, ref, x=xx(-1))

    def dz_step(s):
        for way in (1, -1):
            if s == 0:
                ref = DN.at[z]
            else:
                dz[s, way].wait_recv()
                ref = DN.at[zz(-way * s)]
                if s == NZ // 2 - 1:
                    ref = DN.at[zz(-way * s), pl.ds(0 if way == 1 else NX // 2, NX // 2)]
            if s < NZ // 2:
                dz[s + 1, way] = net.send(ref, ref, z=zz(way))

    def y_own(ch):
        for way in (1, -1):
            ya["T", ch, way] = net.send(tok.at[span(ch)], T.at[me, span(ch)], y=yy(way))
            ya["G", ch, way] = net.send(grd.at[span(ch)], G.at[me, span(ch)], y=yy(way))

    def to_other(name, full, d, ch):
        ref = full.at[slot(d), span(ch)]
        dd[name, d, ch] = net.send(ref, ref, c=other)

    def y_pass(ch):
        ya["T", ch, 1].wait_recv()
        ref = T.at[slot(-1), span(ch)]
        yb["T", ch] = net.send(ref, ref, y=yy(1))
        to_other("T", T, -1, ch)
        ya["G", ch, -1].wait_recv()
        ref = G.at[slot(1), span(ch)]
        yb["G", ch] = net.send(ref, ref, y=yy(-1))
        to_other("G", G, 1, ch)
        ya["G", ch, 1].wait_recv()
        to_other("G", G, -1, ch)
        ya["T", ch, -1].wait_recv()
        to_other("T", T, 1, ch)

    def y_last(ch):
        yb["T", ch].wait_recv()
        to_other("T", T, 2, ch)
        yb["G", ch].wait_recv()
        to_other("G", G, 2, ch)

    def y_ready(ch):
        if ch == 0:
            dd["T"].wait_recv()
            dd["G"].wait_recv()
            locals_[2].wait()
            locals_[3].wait()
        for d in (-1, 1, 2):
            dd["T", d, ch].wait_recv()
            dd["G", d, ch].wait_recv()

    def norm(ch):
        total = jnp.zeros((rows, 128), F32)
        for k in range(NY * NC):
            t = T[k, span(ch)].astype(F32)
            total = total + lanes_summed(t * t)
        inv = lax.rsqrt(jnp.sum(total, axis=1, keepdims=True) / model + 1e-06)
        INV[span(ch)] = inv
        for k in range(NY * NC):
            t = T[k, span(ch)].astype(F32)
            N[k, span(ch)] = (t * inv * gain[k]).astype(BF16)

    def forward(ch):
        pre = jnp.zeros((rows, 2 * ff), F32)
        gh = jnp.zeros((rows, ff), F32)
        for k in range(NY * NC):
            pre = pre + jnp.dot(
                N[k, span(ch)], GU[k].reshape(wide, 2 * ff), preferred_element_type=F32
            )
            gh = gh + jnp.dot(G[k, span(ch)], DN[k].reshape(wide, ff), preferred_element_type=F32)
        gh = 0.5 * gh
        g, u = pre[:, 0:ff], pre[:, ff : 2 * ff]
        sigma = jax.nn.sigmoid(g)
        active = g * sigma
        H[span(ch)] = (active * u).astype(BF16)
        AB[span(ch), 0:ff] = (gh * u * sigma * (1.0 + g * (1.0 - sigma))).astype(BF16)
        AB[span(ch), ff : 2 * ff] = (gh * active).astype(BF16)

    def weights(d):
        k = zz(d)
        DGU[k] = (factor * turned(N[k], AB[...])).reshape(NX, part, 2 * ff)
        DDN[k] = (0.5 * factor * turned(G[k], H[...])).reshape(NX, part, ff)

    def partial(ch):
        ab = AB[span(ch)]
        inv = INV[span(ch)]
        total = jnp.zeros((rows, 128), F32)
        for k in range(NY * NC):
            v = gain[k] * lax.dot_general(
                ab,
                GU[k].reshape(wide, 2 * ff),
                (((1,), (1,)), ((), ())),
                preferred_element_type=F32,
            )
            V[k] = v
            total = total + lanes_summed(v * (T[k, span(ch)].astype(F32) * inv))
        inner = jnp.sum(total, axis=1, keepdims=True) / model
        for k in range(NY * NC):
            unit = T[k, span(ch)].astype(F32) * inv
            PP[k % NC, k // NC, span(ch)] = (inv * (V[k] - unit * inner)).astype(BF16)

    x1, x2, zs, ds, e1, e2, pc, p1, p2 = {}, {}, {}, {}, {}, {}, {}, {}, {}

    def x_step1(i):
        k = zz(ORDER[i])
        SX1[i, 0] = DGU[k, xx(2), :, gate].astype(BF16)
        SX1[i, 1] = DGU[k, xx(2), :, up].astype(BF16)
        x1[i, 1] = net.send(SX1.at[i, 0], RX1.at[i, 0], x=xx(1))
        x1[i, -1] = net.send(SX1.at[i, 1], RX1.at[i, 1], x=xx(-1))

    def x_step2(i):
        k = zz(ORDER[i])
        x1[i, 1].wait_recv()
        SX2[i, 0, :, gate] = (DGU[k, xx(1), :, gate] + RX1[i, 0].astype(F32)).astype(BF16)
        SX2[i, 0, :, up] = DGU[k, xx(1), :, up].astype(BF16)
        x2[i, 1] = net.send(SX2.at[i, 0], RX2.at[i, 0], x=xx(1))
        x1[i, -1].wait_recv()
        SX2[i, 1, :, gate] = DGU[k, xx(-1), :, gate].astype(BF16)
        SX2[i, 1, :, up] = (DGU[k, xx(-1), :, up] + RX1[i, 1].astype(F32)).astype(BF16)
        x2[i, -1] = net.send(SX2.at[i, 1], RX2.at[i, 1], x=xx(-1))

    def x_sum(i):
        x2[i, 1].wait_recv()
        x2[i, -1].wait_recv()
        return DGU[zz(ORDER[i]), x] + RX2[i, 0].astype(F32) + RX2[i, 1].astype(F32)

    def z_step(i):
        d = ORDER[i]
        value = x_sum(i)
        if d == NZ // 2:
            SZ[0, 0] = value.astype(BF16)
            zs[1, d] = net.send(SZ.at[0, 0, :, gate], RZ.at[0, 0, :, gate], z=zz(1))
            zs[-1, d] = net.send(SZ.at[0, 0, :, up], RZ.at[0, 1, :, up], z=zz(-1))
            return None
        ways = (1, -1) if d == 0 else (1 if d > 0 else -1,)
        for way in ways:
            s, w = NZ // 2 - abs(d), 0 if way == 1 else 1
            zs[way, abs(d) + 1].wait_recv()
            if s == 1:
                cols = gate if way == 1 else up
                XR[...] = value
                XR[:, cols] = XR[:, cols] + RZ[0, w, :, cols].astype(F32)
                value = XR[...]
            else:
                value = value + RZ[s - 1, w].astype(F32)
            if d != 0:
                SZ[s, w] = value.astype(BF16)
                zs[way, abs(d)] = net.send(SZ.at[s, w], RZ.at[s, w], z=zz(way))
        return value

    def d_step(i):
        d = ORDER[i]
        k = zz(d)
        near = NX // 2
        if d == NZ // 2:
            SD[0, 0] = DDN[k].astype(BF16)
            lo, hi = pl.ds(0, near), pl.ds(near, near)
            ds[1, d] = net.send(SD.at[0, 0, lo], RD.at[0, 0, lo], z=zz(1))
            ds[-1, d] = net.send(SD.at[0, 0, hi], RD.at[0, 1, hi], z=zz(-1))
            return
        if d == 0:
            ds[1, 1].wait_recv()
            ds[-1, 1].wait_recv()
            last = NZ // 2 - 1
            FD[...] = DDN[k] + RD[last, 0].astype(F32) + RD[last, 1].astype(F32)
            return
        way = 1 if d > 0 else -1
        s, w = NZ // 2 - abs(d), 0 if way == 1 else 1
        ds[way, abs(d) + 1].wait_recv()
        if s == 1:
            own = pl.ds(near if way == 1 else 0, near)
            sent = pl.ds(0 if way == 1 else near, near)
            SD[s, w, own] = DDN[k, own].astype(BF16)
            SD[s, w, sent] = (DDN[k, sent] + RD[0, w, sent].astype(F32)).astype(BF16)
        else:
            SD[s, w] = (DDN[k] + RD[s - 1, w].astype(F32)).astype(BF16)
        ds[way, abs(d)] = net.send(SD.at[s, w], RD.at[s, w], z=zz(way))

    def e_step1():
        SE1[...] = FD[xx(2)].astype(BF16)
        lo, hi = pl.ds(0, half_part), pl.ds(half_part, half_part)
        e1[1] = net.send(SE1.at[lo], RE1.at[lo], x=xx(1))
        e1[-1] = net.send(SE1.at[hi], RE1.at[hi], x=xx(-1))

    def e_step2():
        lo, hi = pl.ds(0, half_part), pl.ds(half_part, half_part)
        e1[1].wait_recv()
        SE2[0, lo] = (FD[xx(1), lo] + RE1[lo].astype(F32)).astype(BF16)
        SE2[0, hi] = FD[xx(1), hi].astype(BF16)
        e2[1] = net.send(SE2.at[0], RE2.at[0], x=xx(1))
        e1[-1].wait_recv()
        SE2[1, lo] = FD[xx(-1), lo].astype(BF16)
        SE2[1, hi] = (FD[xx(-1), hi] + RE1[hi].astype(F32)).astype(BF16)
        e2[-1] = net.send(SE2.at[1], RE2.at[1], x=xx(-1))

    def e_sum():
        e2[1].wait_recv()
        e2[-1].wait_recv()
        return FD[x] + RE2[0].astype(F32) + RE2[1].astype(F32)

    def p_send(ch):
        pc[ch] = net.send(PP.at[other, :, span(ch)], PR.at[:, span(ch)], c=other)

    def p_pair(ch, d, at, n):
        sub = pl.ds(ch * rows + at, n)
        return PP[c, yy(d), sub].astype(F32) + PR[yy(d), sub].astype(F32)

    def p_step1(ch):
        pc[ch].wait_recv()
        S1[ch] = p_pair(ch, 2, 0, rows).astype(BF16)
        lo, hi = pl.ds(0, half_rows), pl.ds(half_rows, half_rows)
        p1[ch, 1] = net.send(S1.at[ch, lo], R1.at[ch, lo], y=yy(1))
        p1[ch, -1] = net.send(S1.at[ch, hi], R1.at[ch, hi], y=yy(-1))

    def p_step2(ch):
        lo, hi = pl.ds(0, half_rows), pl.ds(half_rows, half_rows)
        p1[ch, 1].wait_recv()
        S2[ch, 0, lo] = (p_pair(ch, 1, 0, half_rows) + R1[ch, lo].astype(F32)).astype(BF16)
        S2[ch, 0, hi] = p_pair(ch, 1, half_rows, half_rows).astype(BF16)
        p2[ch, 1] = net.send(S2.at[ch, 0], R2.at[ch, 0], y=yy(1))
        p1[ch, -1].wait_recv()
        S2[ch, 1, lo] = p_pair(ch, -1, 0, half_rows).astype(BF16)
        S2[ch, 1, hi] = (
            p_pair(ch, -1, half_rows, half_rows) + R1[ch, hi].astype(F32)
        ).astype(BF16)
        p2[ch, -1] = net.send(S2.at[ch, 1], R2.at[ch, 1], y=yy(-1))

    def p_sum(ch):
        p2[ch, 1].wait_recv()
        p2[ch, -1].wait_recv()
        total = p_pair(ch, 0, 0, rows) + R2[ch, 0].astype(F32) + R2[ch, 1].astype(F32)
        out_in[span(ch)] = (grd[span(ch)].astype(F32) + total).astype(BF16)

    for way in (1, -1):
        gz[1, way] = net.send(wgu, GU.at[z, x], z=zz(way))
        dx[way] = net.send(wdn, DN.at[z, x], x=xx(way))
    gx_send(0, wgu)
    y_own(0)
    dd["T"] = net.send(tok, T.at[me], c=other)
    dd["G"] = net.send(grd, G.at[me], c=other)
    y_own(1)
    locals_[0].wait()
    locals_[1].wait()
    dx_pass()
    gz_step(1)
    gx_pass(0)
    dxf[1].wait_recv()
    dxf[-1].wait_recv()
    dz_step(0)
    y_pass(0)
    y_own(2)
    gz_step(2)
    gx_pass(-1)
    gx_pass(1)
    dz_step(1)
    y_pass(1)
    y_own(3)
    gz_step(3)
    gx_pass(-2)
    gx_pass(2)
    dz_step(2)
    y_last(0)
    y_ready(0)
    norm(0)
    gz_step(4)
    y_pass(2)
    gx_pass(-3)
    gx_pass(3)
    dz_step(3)
    y_last(1)
    y_ready(1)
    norm(1)
    gx_pass(4)
    y_pass(3)
    dz_step(4)
    for d in (0, -1, 1, -2, 2, -3, 3, 4):
        gxf[d, 1].wait_recv()
        gxf[d, -1].wait_recv()
    forward(0)
    y_last(2)
    y_ready(2)
    norm(2)
    forward(1)
    y_last(3)
    y_ready(3)
    norm(3)
    forward(2)
    forward(3)

    steps = len(ORDER)
    for i in range(steps):
        weights(ORDER[i])
        x_step1(i)
        d_step(i)
        if i >= 1:
            x_step2(i - 1)
        if i % 2 == 0:
            partial(i // 2)
            p_send(i // 2)
        else:
            p_step1(i // 2)
            if i >= 3:
                p_step2(i // 2 - 1)
        if i >= 2:
            z_step(i - 2)
    x_step2(steps - 1)
    e_step1()
    p_step2(CHUNKS - 1)
    z_step(steps - 2)
    e_step2()
    for ch in range(CHUNKS - 1):
        p_sum(ch)
    down = e_sum()
    out_dn[...] = down
    both = z_step(steps - 1)
    out_gu[...] = both
    p_sum(CHUNKS - 1)

    squares = jnp.concatenate(
        [jnp.sum(both * both, axis=0, keepdims=True), jnp.sum(down * down, axis=0, keepdims=True)],
        axis=1,
    )
    QX[x] = squares
    sent = [net.send(QX.at[x], QX.at[x], x=xx(d)) for d in range(1, NX)]
    for copy in sent:
        copy.wait_recv()
    total = QX[0]
    for at in range(1, NX):
        total = total + QX[at]
    QZ[z] = total
    sent = [net.send(QZ.at[z], QZ.at[z], z=zz(d)) for d in range(1, NZ)]
    for copy in sent:
        copy.wait_recv()
    total = QZ[0]
    for at in range(1, NZ):
        total = total + QZ[at]
    out_sq[...] = total / model
    assert len(net.copies) == COPIES, len(net.copies)
    net.finish()


def on_device(tokens, grad_out, norm_gain, gate_weight, up_weight, down_weight):
    n, wide = tokens.shape
    ff, part = gate_weight.shape
    blocks = NY * NC
    rows = n // CHUNKS
    wgu = jnp.concatenate([gate_weight, up_weight], axis=0).T
    wdn = down_weight.T
    gain = norm_gain.reshape(blocks, 1, wide)
    vm = pl.BlockSpec(memory_space=pltpu.VMEM)
    half = NZ // 2
    scratch = [
        ((blocks, n, wide), BF16),
        ((blocks, n, wide), BF16),
        ((blocks, n, wide), BF16),
        ((NZ, NX, part, 2 * ff), BF16),
        ((NZ, NX, part, ff), BF16),
        ((n, 2 * ff), BF16),
        ((n, ff), BF16),
        ((n, 1), F32),
        ((blocks, rows, wide), F32),
        ((NZ, NX, part, 2 * ff), F32),
        ((NZ, NX, part, ff), F32),
        ((NZ, 2, part, ff), BF16),
        ((NZ, 2, part, ff), BF16),
        ((NZ, 2, part, 2 * ff), BF16),
        ((NZ, 2, part, 2 * ff), BF16),
        ((part, 2 * ff), F32),
        ((half, 2, part, 2 * ff), BF16),
        ((half, 2, part, 2 * ff), BF16),
        ((half, 2, NX, part, ff), BF16),
        ((half, 2, NX, part, ff), BF16),
        ((NX, part, ff), F32),
        ((part, ff), BF16),
        ((part, ff), BF16),
        ((2, part, ff), BF16),
        ((2, part, ff), BF16),
        ((NC, NY, n, wide), BF16),
        ((NY, n, wide), BF16),
        ((CHUNKS, rows, wide), BF16),
        ((CHUNKS, rows, wide), BF16),
        ((CHUNKS, 2, rows, wide), BF16),
        ((CHUNKS, 2, rows, wide), BF16),
        ((NX, 1, 3 * ff), F32),
        ((NZ, 1, 3 * ff), F32),
    ]
    grad_in, grad_gu, grad_dn, squares = pl.pallas_call(
        kernel,
        out_shape=(
            jax.ShapeDtypeStruct((n, wide), BF16),
            jax.ShapeDtypeStruct((part, 2 * ff), F32),
            jax.ShapeDtypeStruct((part, ff), F32),
            jax.ShapeDtypeStruct((1, 3 * ff), F32),
        ),
        in_specs=[vm] * 5,
        out_specs=(vm,) * 4,
        scratch_shapes=[pltpu.VMEM(shape, dtype) for shape, dtype in scratch]
        + [
            pltpu.SemaphoreType.DMA((COPIES,)),
            pltpu.SemaphoreType.DMA((COPIES,)),
            pltpu.SemaphoreType.DMA((4,)),
        ],
        compiler_params=pltpu.CompilerParams(
            collective_id=0, has_side_effects=True, vmem_limit_bytes=67043328
        ),
        name="ffn_backward",
    )(tokens, grad_out, gain, wgu, wdn)
    return (
        grad_in,
        grad_gu[:, :ff].T,
        grad_gu[:, ff:].T,
        grad_dn.T,
        squares.reshape(3, ff),
    )


def solution(mesh):
    split = Mesh(mesh.devices.reshape(NZ, NX, NY, NC), FS + TP)
    return jax.shard_map(
        on_device,
        mesh=split,
        in_specs=(P(FS, TP), P(FS, TP), P(), P(TP, FS), P(TP, FS), P(TP, FS)),
        out_specs=(P(FS, TP), P(TP, FS), P(TP, FS), P(TP, FS), P(None, TP)),
        check_vma=False,
    )
```

```python
import jax
import jax.numpy as jnp
from jax import lax
from jax.experimental import pallas as pl
from jax.experimental.pallas import tpu as pltpu
from jax.sharding import Mesh
from jax.sharding import PartitionSpec as P

FS = ("z", "x")
TP = ("y", "c")
NZ, NX, NY, NC = 8, 4, 4, 2
F32, BF16 = jnp.float32, jnp.bfloat16
CHUNKS = 4
COPIES = 196
SPANS = ((0, 256), (256, 256), (512, 256), (768, 128), (896, 128))
ORDER = (4, 3, -3, 2, -2, 1, -1, 0)


class Net:
    def __init__(self, send_sems, recv_sems):
        self.send_sems, self.recv_sems, self.copies = send_sems, recv_sems, []

    def send(self, src, dst, **to):
        at = len(self.copies)
        copy = pltpu.make_async_remote_copy(
            src_ref=src,
            dst_ref=dst,
            send_sem=self.send_sems.at[at],
            recv_sem=self.recv_sems.at[at],
            device_id=to,
            device_id_type=pl.DeviceIdType.MESH,
        )
        copy.start()
        self.copies.append(copy)
        return copy

    def finish(self):
        for copy in self.copies:
            copy.wait_send()


def lanes_summed(v):
    total = v[:, 0:128]
    for at in range(128, v.shape[1], 128):
        total = total + v[:, at : at + 128]
    return total


def turned(left, right):
    return lax.dot_general(left, right, (((0,), (0,)), ((), ())), preferred_element_type=F32)


def kernel(
    tok, grd, gain, wg, wu, wd,
    out_in, out_g, out_u, out_d, out_sq,
    T, G, N, GU, DN, AB, H, INV, V, DGU, DDN,
    SX1, RX1, SX2, RX2, XR, SZ, RZ, SD, RD, FD, SE1, RE1, SE2, RE2,
    PP, PR, S1, R1, S2, R2, QX, QZ, IN, LG, LU, LD,
    send_sems, recv_sems, local_sems,
):
    z, x, y, c = (lax.axis_index(a) for a in ("z", "x", "y", "c"))
    zz = lambda d: lax.rem(z + (d + NZ), NZ)
    xx = lambda d: lax.rem(x + (d + NX), NX)
    yy = lambda d: lax.rem(y + (d + NY), NY)
    other = 1 - c
    me = y * NC + c
    slot = lambda d: yy(d) * NC + c
    tokens = tok.shape[0]
    rows = tokens // CHUNKS
    wide = tok.shape[1]
    part, ff = wd.shape
    model = wide * NY * NC
    half_part, half_rows = part // 2, rows // 2
    gate, up = pl.ds(0, ff), pl.ds(ff, ff)
    factor = (tokens * NZ * NX) ** (-0.5)
    span = lambda ch: pl.ds(ch * rows, rows)
    some = lambda ch: pl.ds(*SPANS[ch])

    barrier = pltpu.get_barrier_semaphore()
    peers = [{a: p} for a, n in (("z", zz), ("x", xx), ("y", yy)) for p in (n(1), n(-1))]
    peers += [{"c": other}]
    for peer in peers:
        pl.semaphore_signal(barrier, inc=1, device_id=peer, device_id_type=pl.DeviceIdType.MESH)
    loads = (
        (wg, GU.at[z, x, :, gate]),
        (wu, GU.at[z, x, :, up]),
        (wd, DN.at[z, x]),
        (tok, T.at[me]),
        (grd, G.at[me]),
    )
    locals_ = [
        pltpu.make_async_copy(src, dst, local_sems.at[i]) for i, (src, dst) in enumerate(loads)
    ]
    for copy in locals_:
        copy.start()
    for copy in locals_:
        copy.wait()
    pl.semaphore_wait(barrier, len(peers))
    net = Net(send_sems, recv_sems)

    gz, gx, gxf, dx, dxf, dz, ya, yb, dd = {}, {}, {}, {}, {}, {}, {}, {}, {}

    def gx_send(d, src):
        gx[d, 1] = net.send(src, GU.at[zz(d), x], x=xx(1))
        gx[d, -1] = net.send(src, GU.at[zz(d), x], x=xx(-1))

    def gx_pass(d):
        gx[d, 1].wait_recv()
        ref = GU.at[zz(d), xx(-1), :, gate]
        gxf[d, 1] = net.send(ref, ref, x=xx(1))
        gx[d, -1].wait_recv()
        ref = GU.at[zz(d), xx(1), :, up]
        gxf[d, -1] = net.send(ref, ref, x=xx(-1))

    def gz_step(s):
        for way in (1, -1):
            gz[s, way].wait_recv()
            if s < NZ // 2:
                ref = GU.at[zz(-way * s), x]
                if s == NZ // 2 - 1:
                    ref = GU.at[zz(-way * s), x, :, gate if way == 1 else up]
                gz[s + 1, way] = net.send(ref, ref, z=zz(way))
        if s < NZ // 2:
            gx_send(-s, GU.at[zz(-s), x])
            gx_send(s, GU.at[zz(s), x])
        else:
            gx_send(s, GU.at[zz(s), x])

    def dx_pass():
        dx[1].wait_recv()
        ref = DN.at[z, xx(-1), pl.ds(0, half_part)]
        dxf[1] = net.send(ref, ref, x=xx(1))
        dx[-1].wait_recv()
        ref = DN.at[z, xx(1), pl.ds(half_part, half_part)]
        dxf[-1] = net.send(ref, ref, x=xx(-1))

    def dz_step(s):
        for way in (1, -1):
            if s == 0:
                ref = DN.at[z]
            else:
                dz[s, way].wait_recv()
                ref = DN.at[zz(-way * s)]
                if s == NZ // 2 - 1:
                    ref = DN.at[zz(-way * s), pl.ds(0 if way == 1 else NX // 2, NX // 2)]
            if s < NZ // 2:
                dz[s + 1, way] = net.send(ref, ref, z=zz(way))

    def y_own(ch):
        for way in (1, -1):
            ya["T", ch, way] = net.send(T.at[me, some(ch)], T.at[me, some(ch)], y=yy(way))
            ya["G", ch, way] = net.send(G.at[me, some(ch)], G.at[me, some(ch)], y=yy(way))

    def to_other(name, full, d, ch):
        ref = full.at[slot(d), some(ch)]
        dd[name, d, ch] = net.send(ref, ref, c=other)

    def y_pass(ch):
        ya["T", ch, 1].wait_recv()
        ref = T.at[slot(-1), some(ch)]
        yb["T", ch] = net.send(ref, ref, y=yy(1))
        to_other("T", T, -1, ch)
        ya["G", ch, -1].wait_recv()
        ref = G.at[slot(1), some(ch)]
        yb["G", ch] = net.send(ref, ref, y=yy(-1))
        to_other("G", G, 1, ch)
        ya["G", ch, 1].wait_recv()
        to_other("G", G, -1, ch)
        ya["T", ch, -1].wait_recv()
        to_other("T", T, 1, ch)

    def y_last(ch):
        yb["T", ch].wait_recv()
        to_other("T", T, 2, ch)
        yb["G", ch].wait_recv()
        to_other("G", G, 2, ch)

    def y_ready(ch):
        if ch == 0:
            dd["T"].wait_recv()
            dd["G"].wait_recv()
        for d in (-1, 1, 2):
            dd["T", d, ch].wait_recv()
            dd["G", d, ch].wait_recv()

    def norm(ch):
        total = jnp.zeros((SPANS[ch][1], 128), F32)
        for k in range(NY * NC):
            t = T[k, some(ch)].astype(F32)
            total = total + lanes_summed(t * t)
        inv = lax.rsqrt(jnp.sum(total, axis=1, keepdims=True) / model + 1e-06)
        INV[some(ch)] = inv
        for k in range(NY * NC):
            t = T[k, some(ch)].astype(F32)
            N[k, some(ch)] = (t * inv * gain[k]).astype(BF16)

    def forward(ch):
        pre = jnp.zeros((SPANS[ch][1], 2 * ff), F32)
        gh = jnp.zeros((SPANS[ch][1], ff), F32)
        for k in range(NY * NC):
            pre = pre + jnp.dot(
                N[k, some(ch)], GU[k].reshape(wide, 2 * ff), preferred_element_type=F32
            )
            gh = gh + jnp.dot(G[k, some(ch)], DN[k].reshape(wide, ff), preferred_element_type=F32)
        gh = 0.5 * gh
        g, u = pre[:, 0:ff], pre[:, ff : 2 * ff]
        sigma = jax.nn.sigmoid(g)
        active = g * sigma
        H[some(ch)] = (active * u).astype(BF16)
        AB[some(ch), 0:ff] = (gh * u * sigma * (1.0 + g * (1.0 - sigma))).astype(BF16)
        AB[some(ch), ff : 2 * ff] = (gh * active).astype(BF16)

    def weights(d):
        k = zz(d)
        DGU[k] = (factor * turned(N[k], AB[...])).reshape(NX, part, 2 * ff)

    def downs(d):
        k = zz(d)
        DDN[k] = (0.5 * factor * turned(G[k], H[...])).reshape(NX, part, ff)

    def partial(ch):
        ab = AB[span(ch)]
        inv = INV[span(ch)]
        total = jnp.zeros((rows, 128), F32)
        for k in range(NY * NC):
            v = gain[k] * lax.dot_general(
                ab,
                GU[k].reshape(wide, 2 * ff),
                (((1,), (1,)), ((), ())),
                preferred_element_type=F32,
            )
            V[k] = v
            total = total + lanes_summed(v * (T[k, span(ch)].astype(F32) * inv))
        inner = jnp.sum(total, axis=1, keepdims=True) / model
        for k in range(NY * NC):
            unit = T[k, span(ch)].astype(F32) * inv
            PP[k % NC, k // NC, span(ch)] = (inv * (V[k] - unit * inner)).astype(BF16)

    x1, x2, zs, ds, e1, e2, pc, p1, p2 = {}, {}, {}, {}, {}, {}, {}, {}, {}

    def x_step1(i):
        k = zz(ORDER[i])
        SX1[i, 0] = DGU[k, xx(2), :, gate].astype(BF16)
        SX1[i, 1] = DGU[k, xx(2), :, up].astype(BF16)
        x1[i, 1] = net.send(SX1.at[i, 0], RX1.at[i, 0], x=xx(1))
        x1[i, -1] = net.send(SX1.at[i, 1], RX1.at[i, 1], x=xx(-1))

    def x_step2(i):
        k = zz(ORDER[i])
        x1[i, 1].wait_recv()
        SX2[i, 0, :, gate] = (DGU[k, xx(1), :, gate] + RX1[i, 0].astype(F32)).astype(BF16)
        SX2[i, 0, :, up] = DGU[k, xx(1), :, up].astype(BF16)
        x2[i, 1] = net.send(SX2.at[i, 0], RX2.at[i, 0], x=xx(1))
        x1[i, -1].wait_recv()
        SX2[i, 1, :, gate] = DGU[k, xx(-1), :, gate].astype(BF16)
        SX2[i, 1, :, up] = (DGU[k, xx(-1), :, up] + RX1[i, 1].astype(F32)).astype(BF16)
        x2[i, -1] = net.send(SX2.at[i, 1], RX2.at[i, 1], x=xx(-1))

    def x_sum(i):
        x2[i, 1].wait_recv()
        x2[i, -1].wait_recv()
        return DGU[zz(ORDER[i]), x] + RX2[i, 0].astype(F32) + RX2[i, 1].astype(F32)

    def z_step(i):
        d = ORDER[i]
        value = x_sum(i)
        if d == NZ // 2:
            SZ[0, 0] = value.astype(BF16)
            zs[1, d] = net.send(SZ.at[0, 0, :, gate], RZ.at[0, 0, :, gate], z=zz(1))
            zs[-1, d] = net.send(SZ.at[0, 0, :, up], RZ.at[0, 1, :, up], z=zz(-1))
            return None
        ways = (1, -1) if d == 0 else (1 if d > 0 else -1,)
        for way in ways:
            s, w = NZ // 2 - abs(d), 0 if way == 1 else 1
            zs[way, abs(d) + 1].wait_recv()
            if s == 1:
                cols = gate if way == 1 else up
                XR[...] = value
                XR[:, cols] = XR[:, cols] + RZ[0, w, :, cols].astype(F32)
                value = XR[...]
            else:
                value = value + RZ[s - 1, w].astype(F32)
            if d != 0:
                SZ[s, w] = value.astype(BF16)
                zs[way, abs(d)] = net.send(SZ.at[s, w], RZ.at[s, w], z=zz(way))
        return value

    def d_step(i):
        d = ORDER[i]
        k = zz(d)
        near = NX // 2
        if d == NZ // 2:
            SD[0, 0] = DDN[k].astype(BF16)
            lo, hi = pl.ds(0, near), pl.ds(near, near)
            ds[1, d] = net.send(SD.at[0, 0, lo], RD.at[0, 0, lo], z=zz(1))
            ds[-1, d] = net.send(SD.at[0, 0, hi], RD.at[0, 1, hi], z=zz(-1))
            return
        if d == 0:
            ds[1, 1].wait_recv()
            ds[-1, 1].wait_recv()
            last = NZ // 2 - 1
            FD[...] = DDN[k] + RD[last, 0].astype(F32) + RD[last, 1].astype(F32)
            return
        way = 1 if d > 0 else -1
        s, w = NZ // 2 - abs(d), 0 if way == 1 else 1
        ds[way, abs(d) + 1].wait_recv()
        if s == 1:
            own = pl.ds(near if way == 1 else 0, near)
            sent = pl.ds(0 if way == 1 else near, near)
            SD[s, w, own] = DDN[k, own].astype(BF16)
            SD[s, w, sent] = (DDN[k, sent] + RD[0, w, sent].astype(F32)).astype(BF16)
        else:
            SD[s, w] = (DDN[k] + RD[s - 1, w].astype(F32)).astype(BF16)
        ds[way, abs(d)] = net.send(SD.at[s, w], RD.at[s, w], z=zz(way))

    def e_step1():
        SE1[...] = FD[xx(2)].astype(BF16)
        lo, hi = pl.ds(0, half_part), pl.ds(half_part, half_part)
        e1[1] = net.send(SE1.at[lo], RE1.at[lo], x=xx(1))
        e1[-1] = net.send(SE1.at[hi], RE1.at[hi], x=xx(-1))

    def e_step2():
        lo, hi = pl.ds(0, half_part), pl.ds(half_part, half_part)
        e1[1].wait_recv()
        SE2[0, lo] = (FD[xx(1), lo] + RE1[lo].astype(F32)).astype(BF16)
        SE2[0, hi] = FD[xx(1), hi].astype(BF16)
        e2[1] = net.send(SE2.at[0], RE2.at[0], x=xx(1))
        e1[-1].wait_recv()
        SE2[1, lo] = FD[xx(-1), lo].astype(BF16)
        SE2[1, hi] = (FD[xx(-1), hi] + RE1[hi].astype(F32)).astype(BF16)
        e2[-1] = net.send(SE2.at[1], RE2.at[1], x=xx(-1))

    def e_sum():
        e2[1].wait_recv()
        e2[-1].wait_recv()
        return FD[x] + RE2[0].astype(F32) + RE2[1].astype(F32)

    def p_send(ch):
        pc[ch] = net.send(PP.at[other, :, span(ch)], PR.at[:, span(ch)], c=other)

    def p_pair(ch, d, at, n):
        sub = pl.ds(ch * rows + at, n)
        return PP[c, yy(d), sub].astype(F32) + PR[yy(d), sub].astype(F32)

    def p_step1(ch):
        pc[ch].wait_recv()
        S1[ch] = p_pair(ch, 2, 0, rows).astype(BF16)
        lo, hi = pl.ds(0, half_rows), pl.ds(half_rows, half_rows)
        p1[ch, 1] = net.send(S1.at[ch, lo], R1.at[ch, lo], y=yy(1))
        p1[ch, -1] = net.send(S1.at[ch, hi], R1.at[ch, hi], y=yy(-1))

    def p_step2(ch):
        lo, hi = pl.ds(0, half_rows), pl.ds(half_rows, half_rows)
        p1[ch, 1].wait_recv()
        S2[ch, 0, lo] = (p_pair(ch, 1, 0, half_rows) + R1[ch, lo].astype(F32)).astype(BF16)
        S2[ch, 0, hi] = p_pair(ch, 1, half_rows, half_rows).astype(BF16)
        p2[ch, 1] = net.send(S2.at[ch, 0], R2.at[ch, 0], y=yy(1))
        p1[ch, -1].wait_recv()
        S2[ch, 1, lo] = p_pair(ch, -1, 0, half_rows).astype(BF16)
        S2[ch, 1, hi] = (
            p_pair(ch, -1, half_rows, half_rows) + R1[ch, hi].astype(F32)
        ).astype(BF16)
        p2[ch, -1] = net.send(S2.at[ch, 1], R2.at[ch, 1], y=yy(-1))

    stores = []

    def store(src, dst):
        copy = pltpu.make_async_copy(src, dst, local_sems.at[len(loads) + len(stores)])
        copy.start()
        stores.append(copy)

    def p_sum(ch):
        p2[ch, 1].wait_recv()
        p2[ch, -1].wait_recv()
        total = p_pair(ch, 0, 0, rows) + R2[ch, 0].astype(F32) + R2[ch, 1].astype(F32)
        IN[span(ch)] = total
        store(IN.at[span(ch)], out_in.at[span(ch)])

    def begin():
        for way in (1, -1):
            gz[1, way] = net.send(GU.at[z, x], GU.at[z, x], z=zz(way))
            dx[way] = net.send(DN.at[z, x], DN.at[z, x], x=xx(way))
        gx_send(0, GU.at[z, x])
        y_own(0)
        dd["T"] = net.send(T.at[me], T.at[me], c=other)
        dd["G"] = net.send(G.at[me], G.at[me], c=other)
        y_own(1)

    def e_finish():
        down = e_sum()
        LD[...] = down
        store(LD, out_d)
        QX[x, :, pl.ds(2 * ff, ff)] = jnp.sum(down * down, axis=0, keepdims=True)

    def z_finish():
        both = z_step(steps - 1)
        LG[...] = both[:, 0:ff]
        LU[...] = both[:, ff : 2 * ff]
        store(LG, out_g)
        store(LU, out_u)
        QX[x, :, pl.ds(0, 2 * ff)] = jnp.sum(both * both, axis=0, keepdims=True)

    def q_x():
        sent = [net.send(QX.at[x], QX.at[x], x=xx(d)) for d in (2, 1, 3)]
        for copy in sent:
            copy.wait_recv()
        total = QX[0]
        for at in range(1, NX):
            total = total + QX[at]
        QZ[z] = total

    def q_z():
        sent = [net.send(QZ.at[z], QZ.at[z], z=zz(d)) for d in (4, 3, 5, 2, 6, 1, 7)]
        for copy in sent:
            copy.wait_recv()
        total = QZ[0]
        for at in range(1, NZ):
            total = total + QZ[at]
        total = total / model
        for at in range(3):
            out_sq[pl.ds(at, 1)] = total[:, at * ff : (at + 1) * ff]

    def finish():
        assert len(net.copies) == COPIES, len(net.copies)
        net.finish()
        for copy in stores:
            copy.wait()

    steps = len(ORDER)
    begin()
    dx_pass()
    gz_step(1)
    gx_pass(0)
    dxf[1].wait_recv()
    dxf[-1].wait_recv()
    dz_step(0)
    y_pass(0)
    y_own(2)
    gz_step(2)
    gx_pass(-1)
    gx_pass(1)
    dz_step(1)
    y_pass(1)
    y_own(3)
    y_own(4)
    gz_step(3)
    gx_pass(-2)
    gx_pass(2)
    dz_step(2)
    y_last(0)
    y_ready(0)
    norm(0)
    gz_step(4)
    y_pass(2)
    gx_pass(-3)
    gx_pass(3)
    dz_step(3)
    y_last(1)
    y_ready(1)
    norm(1)
    gx_pass(4)
    y_pass(3)
    dz_step(4)
    for d in (0, -1, 1, -2, 2, -3, 3, 4):
        gxf[d, 1].wait_recv()
        gxf[d, -1].wait_recv()
    forward(0)
    y_pass(4)
    y_last(2)
    y_ready(2)
    norm(2)
    forward(1)
    y_last(3)
    y_ready(3)
    norm(3)
    forward(2)
    y_last(4)
    forward(3)
    y_ready(4)
    norm(4)
    forward(4)

    downs(ORDER[0])
    d_step(0)
    for i in range(steps):
        if i in (3, 5):
            d_step(i)
            d_step(i + 1)
        if i == 7:
            d_step(i)
            e_step1()
        weights(ORDER[i])
        x_step1(i)
        if i >= 1:
            x_step2(i - 1)
        if i < CHUNKS:
            partial(i)
            p_send(i)
        if i == 1:
            d_step(1)
            d_step(2)
        for j in (2 * i + 1, 2 * i + 2):
            if j < steps:
                downs(ORDER[j])
        if 1 <= i <= CHUNKS:
            p_step1(i - 1)
        if 3 <= i < CHUNKS + 3:
            p_step2(i - 3)
        if i >= 5:
            p_sum(i - 5)
        if i >= 2:
            z_step(i - 2)
    x_step2(steps - 1)
    z_step(steps - 2)
    e_step2()
    p_sum(CHUNKS - 1)
    z_finish()
    e_finish()
    q_x()
    q_z()
    finish()


def on_device(tokens, grad_out, norm_gain, gate_weight, up_weight, down_weight):
    n, wide = tokens.shape
    ff, part = gate_weight.shape
    blocks = NY * NC
    rows = n // CHUNKS
    gain = norm_gain.reshape(blocks, 1, wide)
    vm = pl.BlockSpec(memory_space=pltpu.VMEM)
    hbm = pl.BlockSpec(memory_space=pl.ANY)
    half = NZ // 2
    scratch = [
        ((blocks, n, wide), BF16),
        ((blocks, n, wide), BF16),
        ((blocks, n, wide), BF16),
        ((NZ, NX, part, 2 * ff), BF16),
        ((NZ, NX, part, ff), BF16),
        ((n, 2 * ff), BF16),
        ((n, ff), BF16),
        ((n, 1), F32),
        ((blocks, rows, wide), F32),
        ((NZ, NX, part, 2 * ff), F32),
        ((NZ, NX, part, ff), F32),
        ((NZ, 2, part, ff), BF16),
        ((NZ, 2, part, ff), BF16),
        ((NZ, 2, part, 2 * ff), BF16),
        ((NZ, 2, part, 2 * ff), BF16),
        ((part, 2 * ff), F32),
        ((half, 2, part, 2 * ff), BF16),
        ((half, 2, part, 2 * ff), BF16),
        ((half, 2, NX, part, ff), BF16),
        ((half, 2, NX, part, ff), BF16),
        ((NX, part, ff), F32),
        ((part, ff), BF16),
        ((part, ff), BF16),
        ((2, part, ff), BF16),
        ((2, part, ff), BF16),
        ((NC, NY, n, wide), BF16),
        ((NY, n, wide), BF16),
        ((CHUNKS, rows, wide), BF16),
        ((CHUNKS, rows, wide), BF16),
        ((CHUNKS, 2, rows, wide), BF16),
        ((CHUNKS, 2, rows, wide), BF16),
        ((NX, 1, 3 * ff), F32),
        ((NZ, 1, 3 * ff), F32),
        ((n, wide), F32),
        ((part, ff), F32),
        ((part, ff), F32),
        ((part, ff), F32),
    ]
    grad = jax.ShapeDtypeStruct((part, ff), F32)
    total, grad_gate, grad_up, grad_down, squares = pl.pallas_call(
        kernel,
        out_shape=(
            jax.ShapeDtypeStruct((n, wide), F32),
            grad,
            grad,
            grad,
            jax.ShapeDtypeStruct((3, ff), F32),
        ),
        in_specs=[hbm, hbm, vm, hbm, hbm, hbm],
        out_specs=(hbm, hbm, hbm, hbm, vm),
        scratch_shapes=[pltpu.VMEM(shape, dtype) for shape, dtype in scratch]
        + [
            pltpu.SemaphoreType.DMA((COPIES,)),
            pltpu.SemaphoreType.DMA((COPIES,)),
            pltpu.SemaphoreType.DMA((12,)),
        ],
        compiler_params=pltpu.CompilerParams(
            collective_id=0, has_side_effects=True, vmem_limit_bytes=67043328
        ),
        name="ffn_backward",
    )(tokens, grad_out, gain, gate_weight.T, up_weight.T, down_weight.T)
    grad_in = (grad_out.astype(F32) + total).astype(BF16)
    return grad_in, grad_gate.T, grad_up.T, grad_down.T, squares


def solution(mesh):
    split = Mesh(mesh.devices.reshape(NZ, NX, NY, NC), FS + TP)
    return jax.shard_map(
        on_device,
        mesh=split,
        in_specs=(P(FS, TP), P(FS, TP), P(), P(TP, FS), P(TP, FS), P(TP, FS)),
        out_specs=(P(FS, TP), P(TP, FS), P(TP, FS), P(TP, FS), P(None, TP)),
        check_vma=False,
    )
```

```python
import jax
import jax.numpy as jnp
from jax import lax
from jax.experimental import pallas as pl
from jax.experimental.pallas import tpu as pltpu
from jax.sharding import Mesh
from jax.sharding import PartitionSpec as P

FS = ("z", "x")
TP = ("y", "c")
NZ, NX, NY, NC = 8, 4, 4, 2
F32, BF16 = jnp.float32, jnp.bfloat16
CHUNKS = 4
ARRIVALS = 139
TURNS = 56
SPANS = ((0, 256), (256, 256), (512, 256), (768, 128), (896, 128))
ORDER = (4, 3, -3, 2, -2, 1, -1, 0)


class Net:
    def __init__(self, send_sems, recv_sems):
        self.send_sems, self.recv_sems, self.copies = send_sems, recv_sems, []
        self.groups, self.used = {}, 0

    def send(self, src, dst, group=None, **to):
        at = len(self.copies)
        if at >= TURNS:
            self.copies[at - TURNS].wait_send()
        if group is None:
            group = ("one", at)
        if group not in self.groups:
            self.groups[group] = self.used
            self.used += 1
        copy = pltpu.make_async_remote_copy(
            src_ref=src,
            dst_ref=dst,
            send_sem=self.send_sems.at[at % TURNS],
            recv_sem=self.recv_sems.at[self.groups[group]],
            device_id=to,
            device_id_type=pl.DeviceIdType.MESH,
        )
        copy.start()
        self.copies.append(copy)
        return copy

    def arrived(self, group, size):
        pltpu.make_async_copy(size, size, self.recv_sems.at[self.groups[group]]).wait()

    def finish(self):
        for copy in self.copies[-TURNS:]:
            copy.wait_send()


def lanes_summed(v):
    total = v[:, 0:128]
    for at in range(128, v.shape[1], 128):
        total = total + v[:, at : at + 128]
    return total


def turned(left, right):
    return lax.dot_general(left, right, (((0,), (0,)), ((), ())), preferred_element_type=F32)


def kernel(
    tok, grd, gain, wg, wu, wd,
    out_in, out_g, out_u, out_d, out_sq,
    T, G, N, GU, DN, AB, H, INV, V, DGU, DDN,
    SX1, RX1, SX2, RX2, XR, SZ, RZ, SD, RD, FD, SE1, RE1, SE2, RE2,
    PP, PR, S1, R1, S2, R2, QX, QZ, IN, LG, LU, LD, SQ,
    send_sems, recv_sems, local_sems,
):
    z, x, y, c = (lax.axis_index(a) for a in ("z", "x", "y", "c"))
    zz = lambda d: lax.rem(z + (d + NZ), NZ)
    xx = lambda d: lax.rem(x + (d + NX), NX)
    yy = lambda d: lax.rem(y + (d + NY), NY)
    other = 1 - c
    me = y * NC + c
    slot = lambda d: yy(d) * NC + c
    tokens = tok.shape[0]
    rows = tokens // CHUNKS
    wide = tok.shape[1]
    part, ff = wd.shape
    model = wide * NY * NC
    half_part, half_rows = part // 2, rows // 2
    gate, up = pl.ds(0, ff), pl.ds(ff, ff)
    factor = (tokens * NZ * NX) ** (-0.5)
    span = lambda ch: pl.ds(ch * rows, rows)
    some = lambda ch: pl.ds(*SPANS[ch])

    barrier = pltpu.get_barrier_semaphore()
    peers = [{a: p} for a, n in (("z", zz), ("x", xx), ("y", yy)) for p in (n(1), n(-1))]
    peers += [{"c": other}]
    for peer in peers:
        pl.semaphore_signal(barrier, inc=1, device_id=peer, device_id_type=pl.DeviceIdType.MESH)
    head, rest = some(0), pl.ds(SPANS[0][1], tokens - SPANS[0][1])
    loads = (
        (tok.at[head], T.at[me, head]),
        (grd.at[head], G.at[me, head]),
        (wd, DN.at[z, x]),
        (wg, GU.at[z, x, :, gate]),
        (wu, GU.at[z, x, :, up]),
        (tok.at[rest], T.at[me, rest]),
        (grd.at[rest], G.at[me, rest]),
    )
    locals_ = [
        pltpu.make_async_copy(src, dst, local_sems.at[i]) for i, (src, dst) in enumerate(loads)
    ]
    for copy in locals_:
        copy.start()
    pl.semaphore_wait(barrier, len(peers))
    net = Net(send_sems, recv_sems)

    gz, gx, dx, dz, ya, yb = {}, {}, {}, {}, {}, {}

    def gx_send(d, src):
        gx[d, 1] = net.send(src, GU.at[zz(d), x], x=xx(1))
        gx[d, -1] = net.send(src, GU.at[zz(d), x], x=xx(-1))

    def gx_pass(d):
        gx[d, 1].wait_recv()
        ref = GU.at[zz(d), xx(-1), :, gate]
        net.send(ref, ref, "gxf", x=xx(1))
        gx[d, -1].wait_recv()
        ref = GU.at[zz(d), xx(1), :, up]
        net.send(ref, ref, "gxf", x=xx(-1))

    def gz_step(s):
        for way in (1, -1):
            gz[s, way].wait_recv()
            if s < NZ // 2:
                ref = GU.at[zz(-way * s), x]
                if s == NZ // 2 - 1:
                    ref = GU.at[zz(-way * s), x, :, gate if way == 1 else up]
                gz[s + 1, way] = net.send(ref, ref, z=zz(way))
        if s < NZ // 2:
            gx_send(-s, GU.at[zz(-s), x])
            gx_send(s, GU.at[zz(s), x])
        else:
            gx_send(s, GU.at[zz(s), x])

    def dx_pass():
        dx[1].wait_recv()
        ref = DN.at[z, xx(-1), pl.ds(0, half_part)]
        net.send(ref, ref, "dxf", x=xx(1))
        dx[-1].wait_recv()
        ref = DN.at[z, xx(1), pl.ds(half_part, half_part)]
        net.send(ref, ref, "dxf", x=xx(-1))

    def dz_step(s, *pieces):
        for dx_ in pieces:
            for way in (1, -1):
                if s > 0:
                    dz[s, dx_, way].wait_recv()
                ref = DN.at[zz(-way * s), xx(dx_)]
                if s < NZ // 2 - 1:
                    dz[s + 1, dx_, way] = net.send(ref, ref, z=zz(way))
                elif (dx_ in (0, -1)) == (way == 1):
                    net.send(ref, ref, "dz", z=zz(way))

    def y_own(ch):
        for way in (1, -1):
            ya["T", ch, way] = net.send(T.at[me, some(ch)], T.at[me, some(ch)], y=yy(way))
            ya["G", ch, way] = net.send(G.at[me, some(ch)], G.at[me, some(ch)], y=yy(way))

    def to_other(name, full, d, ch):
        ref = full.at[slot(d), some(ch)]
        net.send(ref, ref, ("c", ch), c=other)

    def y_pass(ch):
        ya["T", ch, 1].wait_recv()
        ref = T.at[slot(-1), some(ch)]
        yb["T", ch] = net.send(ref, ref, y=yy(1))
        to_other("T", T, -1, ch)
        ya["G", ch, -1].wait_recv()
        ref = G.at[slot(1), some(ch)]
        yb["G", ch] = net.send(ref, ref, y=yy(-1))
        to_other("G", G, 1, ch)
        ya["G", ch, 1].wait_recv()
        to_other("G", G, -1, ch)
        ya["T", ch, -1].wait_recv()
        to_other("T", T, 1, ch)

    def y_last(ch):
        yb["T", ch].wait_recv()
        to_other("T", T, 2, ch)
        yb["G", ch].wait_recv()
        to_other("G", G, 2, ch)

    def y_ready(ch):
        of_all = 6 * SPANS[ch][1] + (2 * tokens if ch == 0 else 0)
        lots = NY if ch == 0 else 3
        net.arrived(("c", ch), PP.at[0, pl.ds(0, lots), pl.ds(0, of_all // lots)])

    def norm(ch):
        total = jnp.zeros((SPANS[ch][1], 128), F32)
        for k in range(NY * NC):
            t = T[k, some(ch)].astype(F32)
            total = total + lanes_summed(t * t)
        inv = lax.rsqrt(jnp.sum(total, axis=1, keepdims=True) / model + 1e-06)
        INV[some(ch)] = inv
        for k in range(NY * NC):
            t = T[k, some(ch)].astype(F32)
            N[k, some(ch)] = (t * inv * gain[k]).astype(BF16)

    def forward(ch):
        pre = jnp.zeros((SPANS[ch][1], 2 * ff), F32)
        gh = jnp.zeros((SPANS[ch][1], ff), F32)
        for k in range(NY * NC):
            pre = pre + jnp.dot(
                N[k, some(ch)], GU[k].reshape(wide, 2 * ff), preferred_element_type=F32
            )
            gh = gh + jnp.dot(G[k, some(ch)], DN[k].reshape(wide, ff), preferred_element_type=F32)
        gh = 0.5 * gh
        g, u = pre[:, 0:ff], pre[:, ff : 2 * ff]
        sigma = jax.nn.sigmoid(g)
        active = g * sigma
        H[some(ch)] = (active * u).astype(BF16)
        AB[some(ch), 0:ff] = (gh * u * sigma * (1.0 + g * (1.0 - sigma))).astype(BF16)
        AB[some(ch), ff : 2 * ff] = (gh * active).astype(BF16)

    def weights(d):
        k = zz(d)
        DGU[k] = (factor * turned(N[k], AB[...])).reshape(NX, part, 2 * ff)

    def downs(d):
        k = zz(d)
        DDN[k] = (0.5 * factor * turned(G[k], H[...])).reshape(NX, part, ff)

    def partial(ch):
        ab = AB[span(ch)]
        inv = INV[span(ch)]
        total = jnp.zeros((rows, 128), F32)
        for k in range(NY * NC):
            v = gain[k] * lax.dot_general(
                ab,
                GU[k].reshape(wide, 2 * ff),
                (((1,), (1,)), ((), ())),
                preferred_element_type=F32,
            )
            V[k] = v
            total = total + lanes_summed(v * (T[k, span(ch)].astype(F32) * inv))
        inner = jnp.sum(total, axis=1, keepdims=True) / model
        for k in range(NY * NC):
            unit = T[k, span(ch)].astype(F32) * inv
            PP[k % NC, k // NC, span(ch)] = (inv * (V[k] - unit * inner)).astype(BF16)

    zs, ds, pc = {}, {}, {}

    def x_step1(i):
        k = zz(ORDER[i])
        SX1[i, 0] = DGU[k, xx(2), :, gate].astype(BF16)
        SX1[i, 1] = DGU[k, xx(2), :, up].astype(BF16)
        net.send(SX1.at[i, 0], RX1.at[i, 0], ("x1", i), x=xx(1))
        net.send(SX1.at[i, 1], RX1.at[i, 1], ("x1", i), x=xx(-1))

    def x_step2(i):
        k = zz(ORDER[i])
        net.arrived(("x1", i), SX1.at[i])
        SX2[i, 0, :, gate] = (DGU[k, xx(1), :, gate] + RX1[i, 0].astype(F32)).astype(BF16)
        SX2[i, 0, :, up] = DGU[k, xx(1), :, up].astype(BF16)
        net.send(SX2.at[i, 0], RX2.at[i, 0], ("x2", i), x=xx(1))
        SX2[i, 1, :, gate] = DGU[k, xx(-1), :, gate].astype(BF16)
        SX2[i, 1, :, up] = (DGU[k, xx(-1), :, up] + RX1[i, 1].astype(F32)).astype(BF16)
        net.send(SX2.at[i, 1], RX2.at[i, 1], ("x2", i), x=xx(-1))

    def x_sum(i):
        net.arrived(("x2", i), SX2.at[i])
        return DGU[zz(ORDER[i]), x] + RX2[i, 0].astype(F32) + RX2[i, 1].astype(F32)

    def z_step(i):
        d = ORDER[i]
        value = x_sum(i)
        if d == NZ // 2:
            SZ[0, 0] = value.astype(BF16)
            zs[1, d] = net.send(SZ.at[0, 0, :, gate], RZ.at[0, 0, :, gate], z=zz(1))
            zs[-1, d] = net.send(SZ.at[0, 0, :, up], RZ.at[0, 1, :, up], z=zz(-1))
            return None
        ways = (1, -1) if d == 0 else (1 if d > 0 else -1,)
        for way in ways:
            s, w = NZ // 2 - abs(d), 0 if way == 1 else 1
            zs[way, abs(d) + 1].wait_recv()
            if s == 1:
                cols = gate if way == 1 else up
                XR[...] = value
                XR[:, cols] = XR[:, cols] + RZ[0, w, :, cols].astype(F32)
                value = XR[...]
            else:
                value = value + RZ[s - 1, w].astype(F32)
            if d != 0:
                SZ[s, w] = value.astype(BF16)
                zs[way, abs(d)] = net.send(SZ.at[s, w], RZ.at[s, w], z=zz(way))
        return value

    def d_step(d, way, half):
        k, w = zz(d), 0 if way == 1 else 1
        first = half == w
        blocks = pl.ds(half * (NX // 2), NX // 2)
        s = NZ // 2 - abs(d)
        value = DDN[k, blocks]
        if s >= (1 if first else 2):
            ds[way, half, abs(d) + 1].wait_recv()
            value = value + RD[s - 1, w, blocks].astype(F32)
        SD[s, w, blocks] = value.astype(BF16)
        group = "ds" if abs(d) == 1 else None
        ds[way, half, abs(d)] = net.send(
            SD.at[s, w, blocks], RD.at[s, w, blocks], group, z=zz(way)
        )

    def d_both(s, old):
        for way in (1, -1):
            d_step(way * (NZ // 2 - s), way, (0 if way == 1 else 1) if old else (1 if way == 1 else 0))

    def d_sum():
        last = NZ // 2 - 1
        net.arrived("ds", SD.at[last])
        FD[...] = DDN[z] + RD[last, 0].astype(F32) + RD[last, 1].astype(F32)

    def e_step1():
        SE1[...] = FD[xx(2)].astype(BF16)
        lo, hi = pl.ds(0, half_part), pl.ds(half_part, half_part)
        net.send(SE1.at[lo], RE1.at[lo], "e1", x=xx(1))
        net.send(SE1.at[hi], RE1.at[hi], "e1", x=xx(-1))

    def e_step2():
        lo, hi = pl.ds(0, half_part), pl.ds(half_part, half_part)
        net.arrived("e1", SE1)
        SE2[0, lo] = (FD[xx(1), lo] + RE1[lo].astype(F32)).astype(BF16)
        SE2[0, hi] = FD[xx(1), hi].astype(BF16)
        net.send(SE2.at[0], RE2.at[0], "e2", x=xx(1))
        SE2[1, lo] = FD[xx(-1), lo].astype(BF16)
        SE2[1, hi] = (FD[xx(-1), hi] + RE1[hi].astype(F32)).astype(BF16)
        net.send(SE2.at[1], RE2.at[1], "e2", x=xx(-1))

    def e_sum():
        net.arrived("e2", SE2)
        return FD[x] + RE2[0].astype(F32) + RE2[1].astype(F32)

    def p_send(ch):
        pc[ch] = net.send(PP.at[other, :, span(ch)], PR.at[:, span(ch)], c=other)

    def p_pair(ch, d, at, n):
        sub = pl.ds(ch * rows + at, n)
        return PP[c, yy(d), sub].astype(F32) + PR[yy(d), sub].astype(F32)

    def p_step1(ch):
        pc[ch].wait_recv()
        S1[ch] = p_pair(ch, 2, 0, rows).astype(BF16)
        lo, hi = pl.ds(0, half_rows), pl.ds(half_rows, half_rows)
        net.send(S1.at[ch, lo], R1.at[ch, lo], ("p1", ch), y=yy(1))
        net.send(S1.at[ch, hi], R1.at[ch, hi], ("p1", ch), y=yy(-1))

    def p_step2(ch):
        lo, hi = pl.ds(0, half_rows), pl.ds(half_rows, half_rows)
        net.arrived(("p1", ch), S1.at[ch])
        S2[ch, 0, lo] = (p_pair(ch, 1, 0, half_rows) + R1[ch, lo].astype(F32)).astype(BF16)
        S2[ch, 0, hi] = p_pair(ch, 1, half_rows, half_rows).astype(BF16)
        net.send(S2.at[ch, 0], R2.at[ch, 0], ("p2", ch), y=yy(1))
        S2[ch, 1, lo] = p_pair(ch, -1, 0, half_rows).astype(BF16)
        S2[ch, 1, hi] = (
            p_pair(ch, -1, half_rows, half_rows) + R1[ch, hi].astype(F32)
        ).astype(BF16)
        net.send(S2.at[ch, 1], R2.at[ch, 1], ("p2", ch), y=yy(-1))

    stores = []

    def store(src, dst):
        copy = pltpu.make_async_copy(src, dst, local_sems.at[len(loads) + len(stores)])
        copy.start()
        stores.append(copy)

    def p_sum(ch):
        net.arrived(("p2", ch), S2.at[ch])
        total = p_pair(ch, 0, 0, rows) + R2[ch, 0].astype(F32) + R2[ch, 1].astype(F32)
        IN[span(ch)] = (G[me, span(ch)].astype(F32) + total).astype(BF16)
        store(IN.at[span(ch)], out_in.at[span(ch)])

    def begin():
        locals_[0].wait()
        locals_[1].wait()
        y_own(0)
        for copy in locals_[2:5]:
            copy.wait()
        for way in (1, -1):
            gz[1, way] = net.send(GU.at[z, x], GU.at[z, x], z=zz(way))
            dx[way] = net.send(DN.at[z, x], DN.at[z, x], x=xx(way))
        dz_step(0, 0)
        gx_send(0, GU.at[z, x])
        for copy in locals_[5:]:
            copy.wait()
        y_own(1)
        net.send(T.at[me], T.at[me], ("c", 0), c=other)
        net.send(G.at[me], G.at[me], ("c", 0), c=other)

    def e_finish():
        down = e_sum()
        LD[...] = down
        store(LD, out_d)
        QX[x, :, pl.ds(2 * ff, ff)] = jnp.sum(down * down, axis=0, keepdims=True)

    def z_finish():
        both = z_step(steps - 1)
        LG[...] = both[:, 0:ff]
        LU[...] = both[:, ff : 2 * ff]
        store(LG, out_g)
        store(LU, out_u)
        QX[x, :, pl.ds(0, 2 * ff)] = jnp.sum(both * both, axis=0, keepdims=True)

    def q_x():
        for d in (2, 1, 3):
            net.send(QX.at[x], QX.at[x], "qx", x=xx(d))
        p_sum(2)
        net.arrived("qx", QX.at[pl.ds(0, NX - 1)])
        total = QX[0]
        for at in range(1, NX):
            total = total + QX[at]
        QZ[z] = total

    def q_z():
        for d in (4, 3, 5, 2, 6, 1, 7):
            net.send(QZ.at[z], QZ.at[z], "qz", z=zz(d))
        p_sum(3)
        net.arrived("qz", QZ.at[pl.ds(0, NZ - 1)])
        total = QZ[0]
        for at in range(1, NZ):
            total = total + QZ[at]
        total = total / model
        for at in range(3):
            SQ[pl.ds(at, 1)] = total[:, at * ff : (at + 1) * ff]
        store(SQ, out_sq)

    def finish():
        assert net.used == ARRIVALS, net.used
        net.finish()
        for copy in stores:
            copy.wait()

    steps = len(ORDER)
    begin()
    dx_pass()
    gz_step(1)
    dz_step(0, -1, 1)
    gx_pass(0)
    dz_step(1, 0)
    net.arrived("dxf", DN.at[0, 0])
    y_pass(0)
    y_own(2)
    gz_step(2)
    dz_step(0, 2)
    gx_pass(-1)
    dz_step(1, -1, 1)
    gx_pass(1)
    y_pass(1)
    y_own(3)
    y_own(4)
    gz_step(3)
    dz_step(2, 0)
    dz_step(1, 2)
    y_last(0)
    gx_pass(-2)
    gz_step(4)
    gx_pass(2)
    dz_step(2, -1, 1)
    dz_step(3, 0)
    dz_step(2, 2)
    y_pass(2)
    gx_pass(-3)
    gx_pass(3)
    dz_step(3, -1, 1)
    y_last(1)
    dz_step(3, 2)
    y_ready(0)
    norm(0)
    gx_pass(4)
    y_pass(3)
    net.arrived("dz", DN.at[0])
    net.arrived("gxf", DN.at[pl.ds(0, 4)])
    forward(0)
    y_ready(1)
    norm(1)
    y_pass(4)
    forward(1)
    y_last(2)
    y_ready(2)
    norm(2)
    y_last(3)
    forward(2)
    y_last(4)
    y_ready(3)
    norm(3)
    forward(3)
    y_ready(4)
    norm(4)
    forward(4)

    ahead = 3
    weights(ORDER[0])
    x_step1(0)
    downs(ORDER[0])
    d_both(0, True)
    weights(ORDER[1])
    x_step1(1)
    downs(ORDER[1])
    downs(ORDER[2])
    d_both(1, False)
    weights(ORDER[2])
    x_step1(2)
    for i in range(5):
        x_step2(i)
        weights(ORDER[i + ahead])
        x_step1(i + ahead)
        if i == 0:
            downs(ORDER[3])
            downs(ORDER[4])
            d_both(1, True)
        if i == 1:
            d_both(2, False)
        if i == 2:
            downs(ORDER[5])
            downs(ORDER[6])
            d_both(2, True)
        if i == 3:
            d_both(3, False)
        if i == 4:
            downs(ORDER[7])
            d_both(3, True)
        if i >= 2:
            p_step1(i - 2)
        if i < CHUNKS:
            partial(i)
            p_send(i)
        if i >= 1:
            z_step(i - 1)
    x_step2(5)
    p_step1(3)
    p_step2(0)
    x_step2(6)
    z_step(4)
    x_step2(7)
    p_step2(1)
    d_sum()
    e_step1()
    z_step(5)
    p_step2(2)
    z_step(6)
    e_step2()
    p_step2(3)
    p_sum(0)
    p_sum(1)
    z_finish()
    e_finish()
    q_x()
    q_z()
    finish()


def deliver(*refs):
    n = (len(refs) - 2) // 3
    given, taken, held = refs[:n], refs[n : 2 * n], refs[2 * n : 3 * n]
    in_sems, out_sems = refs[3 * n :]
    parts = []
    for src, mid, dst in zip(given, held, taken):
        step = min(src.shape[0], 256)
        for at in range(0, src.shape[0], step):
            sub, i = pl.ds(at, step), len(parts)
            parts.append(
                (
                    pltpu.make_async_copy(src.at[sub], mid.at[sub], in_sems.at[i]),
                    pltpu.make_async_copy(mid.at[sub], dst.at[sub], out_sems.at[i]),
                )
            )
    for load, _ in parts:
        load.start()
    for load, save in parts:
        load.wait()
        save.start()
    for _, save in parts:
        save.wait()


def on_device(tokens, grad_out, norm_gain, gate_weight, up_weight, down_weight):
    n, wide = tokens.shape
    ff, part = gate_weight.shape
    blocks = NY * NC
    rows = n // CHUNKS
    gain = norm_gain.reshape(blocks, 1, wide)
    vm = pl.BlockSpec(memory_space=pltpu.VMEM)
    hbm = pl.BlockSpec(memory_space=pl.ANY)
    half = NZ // 2
    scratch = [
        ((blocks, n, wide), BF16),
        ((blocks, n, wide), BF16),
        ((blocks, n, wide), BF16),
        ((NZ, NX, part, 2 * ff), BF16),
        ((NZ, NX, part, ff), BF16),
        ((n, 2 * ff), BF16),
        ((n, ff), BF16),
        ((n, 1), F32),
        ((blocks, rows, wide), F32),
        ((NZ, NX, part, 2 * ff), F32),
        ((NZ, NX, part, ff), F32),
        ((NZ, 2, part, ff), BF16),
        ((NZ, 2, part, ff), BF16),
        ((NZ, 2, part, 2 * ff), BF16),
        ((NZ, 2, part, 2 * ff), BF16),
        ((part, 2 * ff), F32),
        ((half, 2, part, 2 * ff), BF16),
        ((half, 2, part, 2 * ff), BF16),
        ((half, 2, NX, part, ff), BF16),
        ((half, 2, NX, part, ff), BF16),
        ((NX, part, ff), F32),
        ((part, ff), BF16),
        ((part, ff), BF16),
        ((2, part, ff), BF16),
        ((2, part, ff), BF16),
        ((NC, NY, n, wide), BF16),
        ((NY, n, wide), BF16),
        ((CHUNKS, rows, wide), BF16),
        ((CHUNKS, rows, wide), BF16),
        ((CHUNKS, 2, rows, wide), BF16),
        ((CHUNKS, 2, rows, wide), BF16),
        ((NX, 1, 3 * ff), F32),
        ((NZ, 1, 3 * ff), F32),
        ((n, wide), BF16),
        ((part, ff), F32),
        ((part, ff), F32),
        ((part, ff), F32),
        ((3, ff), F32),
    ]
    grad = jax.ShapeDtypeStruct((part, ff), F32)
    grad_in, grad_gate, grad_up, grad_down, squares = pl.pallas_call(
        kernel,
        out_shape=(
            jax.ShapeDtypeStruct((n, wide), BF16),
            grad,
            grad,
            grad,
            jax.ShapeDtypeStruct((3, ff), F32),
        ),
        in_specs=[hbm, hbm, vm, hbm, hbm, hbm],
        out_specs=(hbm,) * 5,
        scratch_shapes=[pltpu.VMEM(shape, dtype) for shape, dtype in scratch]
        + [
            pltpu.SemaphoreType.DMA((TURNS,)),
            pltpu.SemaphoreType.DMA((ARRIVALS,)),
            pltpu.SemaphoreType.DMA((15,)),
        ],
        compiler_params=pltpu.CompilerParams(
            collective_id=0, has_side_effects=True, vmem_limit_bytes=67043328
        ),
        name="ffn_backward",
    )(tokens, grad_out, gain, gate_weight.T, up_weight.T, down_weight.T)
    found = (grad_in, grad_gate, grad_up, grad_down, squares)
    results = pl.pallas_call(
        deliver,
        out_shape=tuple(jax.ShapeDtypeStruct(a.shape, a.dtype) for a in found),
        in_specs=[hbm] * 5,
        out_specs=(hbm,) * 5,
        scratch_shapes=[pltpu.VMEM(a.shape, a.dtype) for a in found]
        + [pltpu.SemaphoreType.DMA((8,)), pltpu.SemaphoreType.DMA((8,))],
        name="deliver",
    )(*found)
    grad_in, grad_gate, grad_up, grad_down, squares = results
    return grad_in, grad_gate.T, grad_up.T, grad_down.T, squares


def solution(mesh):
    split = Mesh(mesh.devices.reshape(NZ, NX, NY, NC), FS + TP)
    return jax.shard_map(
        on_device,
        mesh=split,
        in_specs=(P(FS, TP), P(FS, TP), P(), P(TP, FS), P(TP, FS), P(TP, FS)),
        out_specs=(P(FS, TP), P(TP, FS), P(TP, FS), P(TP, FS), P(None, TP)),
        check_vma=False,
    )
```

```python
import jax
import jax.numpy as jnp
from jax import lax
from jax.experimental import pallas as pl
from jax.experimental.pallas import tpu as pltpu
from jax.sharding import Mesh
from jax.sharding import PartitionSpec as P

FS = ("z", "x")
TP = ("y", "c")
NZ, NX, NY, NC = 8, 4, 4, 2
F32, BF16 = jnp.float32, jnp.bfloat16
CHUNKS = 4
ARRIVALS = 138
KINDS = 19
SPANS = ((0, 256), (256, 256), (512, 256), (768, 128), (896, 128))
ORDER = (4, 3, -3, 2, -2, 1, -1, 0)


class Net:
    def __init__(self, send_sems, recv_sems):
        self.send_sems, self.recv_sems = send_sems, recv_sems
        self.kinds, self.groups, self.used = [], {}, 0

    def send(self, kind, src, dst, group=None, **to):
        if kind not in self.kinds:
            self.kinds.append(kind)
        if group not in self.groups or group is None:
            self.groups[group] = self.used
            self.used += 1
        copy = pltpu.make_async_remote_copy(
            src_ref=src,
            dst_ref=dst,
            send_sem=self.send_sems.at[self.kinds.index(kind)],
            recv_sem=self.recv_sems.at[self.groups[group]],
            device_id=to,
            device_id_type=pl.DeviceIdType.MESH,
        )
        copy.start()
        return copy

    def arrived(self, group, size):
        pltpu.make_async_copy(size, size, self.recv_sems.at[self.groups[group]]).wait()

    def sent(self, kind, size):
        pltpu.make_async_copy(size, size, self.send_sems.at[self.kinds.index(kind)]).wait()


def lanes_summed(v):
    total = v[:, 0:128]
    for at in range(128, v.shape[1], 128):
        total = total + v[:, at : at + 128]
    return total


def turned(left, right):
    return lax.dot_general(left, right, (((0,), (0,)), ((), ())), preferred_element_type=F32)


def kernel(
    tok, grd, gain, wg, wu, wd,
    out_in, out_g, out_u, out_d, out_sq,
    T, G, N, GU, DN, AB, H, INV, V, DGU, DDN,
    SX1, RX1, SX2, RX2, XR, SZ, RZ, SD, RD, FD, SE1, RE1, SE2, RE2,
    PP, PR, S1, R1, S2, R2, QA, IN, LG, LU, LD, SQ,
    send_sems, recv_sems, local_sems,
):
    z, x, y, c = (lax.axis_index(a) for a in ("z", "x", "y", "c"))
    zz = lambda d: lax.rem(z + (d + NZ), NZ)
    xx = lambda d: lax.rem(x + (d + NX), NX)
    yy = lambda d: lax.rem(y + (d + NY), NY)
    other = 1 - c
    me = y * NC + c
    slot = lambda d: yy(d) * NC + c
    tokens = tok.shape[0]
    rows = tokens // CHUNKS
    wide = tok.shape[1]
    part, ff = wd.shape
    model = wide * NY * NC
    half_part, half_rows = part // 2, rows // 2
    gate, up = pl.ds(0, ff), pl.ds(ff, ff)
    factor = (tokens * NZ * NX) ** (-0.5)
    span = lambda ch: pl.ds(ch * rows, rows)
    some = lambda ch: pl.ds(*SPANS[ch])

    barrier = pltpu.get_barrier_semaphore()
    peers = [{a: p} for a, n in (("z", zz), ("x", xx), ("y", yy)) for p in (n(1), n(-1))]
    peers += [{"c": other}]
    for peer in peers:
        pl.semaphore_signal(barrier, inc=1, device_id=peer, device_id_type=pl.DeviceIdType.MESH)
    head, rest = some(0), pl.ds(SPANS[0][1], tokens - SPANS[0][1])
    loads = (
        (tok.at[head], T.at[me, head]),
        (grd.at[head], G.at[me, head]),
        (wd, DN.at[z, x]),
        (wg, GU.at[z, x, :, gate]),
        (wu, GU.at[z, x, :, up]),
        (tok.at[rest], T.at[me, rest]),
        (grd.at[rest], G.at[me, rest]),
    )
    locals_ = [
        pltpu.make_async_copy(src, dst, local_sems.at[i]) for i, (src, dst) in enumerate(loads)
    ]
    for copy in locals_:
        copy.start()
    pl.semaphore_wait(barrier, len(peers))
    net = Net(send_sems, recv_sems)

    gz, gx, dx, dz, ya, yb = {}, {}, {}, {}, {}, {}

    def gx_send(d, src):
        gx[d, 1] = net.send("gx", src, GU.at[zz(d), x], x=xx(1))
        gx[d, -1] = net.send("gx", src, GU.at[zz(d), x], x=xx(-1))

    def gx_pass(d):
        gx[d, 1].wait_recv()
        ref = GU.at[zz(d), xx(-1), :, gate]
        net.send("gxf", ref, ref, "gxf", x=xx(1))
        gx[d, -1].wait_recv()
        ref = GU.at[zz(d), xx(1), :, up]
        net.send("gxf", ref, ref, "gxf", x=xx(-1))

    def gz_step(s):
        for way in (1, -1):
            gz[s, way].wait_recv()
            if s < NZ // 2:
                ref = GU.at[zz(-way * s), x]
                if s == NZ // 2 - 1:
                    ref = GU.at[zz(-way * s), x, :, gate if way == 1 else up]
                gz[s + 1, way] = net.send("gz", ref, ref, z=zz(way))
        if s < NZ // 2:
            gx_send(-s, GU.at[zz(-s), x])
            gx_send(s, GU.at[zz(s), x])
        else:
            gx_send(s, GU.at[zz(s), x])

    def dx_pass():
        dx[1].wait_recv()
        ref = DN.at[z, xx(-1), pl.ds(0, half_part)]
        net.send("dxf", ref, ref, "dxf", x=xx(1))
        dx[-1].wait_recv()
        ref = DN.at[z, xx(1), pl.ds(half_part, half_part)]
        net.send("dxf", ref, ref, "dxf", x=xx(-1))

    def dz_step(s, *pieces):
        for dx_ in pieces:
            for way in (1, -1):
                if s > 0:
                    dz[s, dx_, way].wait_recv()
                ref = DN.at[zz(-way * s), xx(dx_)]
                if s < NZ // 2 - 1:
                    dz[s + 1, dx_, way] = net.send("dz", ref, ref, z=zz(way))
                elif (dx_ in (0, -1)) == (way == 1):
                    net.send("dz", ref, ref, "dz", z=zz(way))

    def y_own(ch):
        for way in (1, -1):
            ya["T", ch, way] = net.send("ya", T.at[me, some(ch)], T.at[me, some(ch)], y=yy(way))
            ya["G", ch, way] = net.send("ya", G.at[me, some(ch)], G.at[me, some(ch)], y=yy(way))

    def to_other(name, full, d, ch):
        ref = full.at[slot(d), some(ch)]
        net.send("c", ref, ref, ("c", ch), c=other)

    def y_pass(ch):
        ya["T", ch, 1].wait_recv()
        ref = T.at[slot(-1), some(ch)]
        yb["T", ch] = net.send("yb", ref, ref, y=yy(1))
        to_other("T", T, -1, ch)
        ya["G", ch, -1].wait_recv()
        ref = G.at[slot(1), some(ch)]
        yb["G", ch] = net.send("yb", ref, ref, y=yy(-1))
        to_other("G", G, 1, ch)
        ya["G", ch, 1].wait_recv()
        to_other("G", G, -1, ch)
        ya["T", ch, -1].wait_recv()
        to_other("T", T, 1, ch)

    def y_last(ch):
        yb["T", ch].wait_recv()
        to_other("T", T, 2, ch)
        yb["G", ch].wait_recv()
        to_other("G", G, 2, ch)

    def y_ready(ch):
        of_all = 6 * SPANS[ch][1] + (2 * tokens if ch == 0 else 0)
        lots = NY if ch == 0 else 3
        net.arrived(("c", ch), PP.at[0, pl.ds(0, lots), pl.ds(0, of_all // lots)])

    def norm(ch):
        total = jnp.zeros((SPANS[ch][1], 128), F32)
        for k in range(NY * NC):
            t = T[k, some(ch)].astype(F32)
            total = total + lanes_summed(t * t)
        inv = lax.rsqrt(jnp.sum(total, axis=1, keepdims=True) / model + 1e-06)
        INV[some(ch)] = inv
        for k in range(NY * NC):
            t = T[k, some(ch)].astype(F32)
            N[k, some(ch)] = (t * inv * gain[k]).astype(BF16)

    def forward(ch):
        pre = jnp.zeros((SPANS[ch][1], 2 * ff), F32)
        gh = jnp.zeros((SPANS[ch][1], ff), F32)
        for k in range(NY * NC):
            pre = pre + jnp.dot(
                N[k, some(ch)], GU[k].reshape(wide, 2 * ff), preferred_element_type=F32
            )
            gh = gh + jnp.dot(G[k, some(ch)], DN[k].reshape(wide, ff), preferred_element_type=F32)
        gh = 0.5 * gh
        g, u = pre[:, 0:ff], pre[:, ff : 2 * ff]
        sigma = jax.nn.sigmoid(g)
        active = g * sigma
        H[some(ch)] = (active * u).astype(BF16)
        AB[some(ch), 0:ff] = (gh * u * sigma * (1.0 + g * (1.0 - sigma))).astype(BF16)
        AB[some(ch), ff : 2 * ff] = (gh * active).astype(BF16)

    def weights(d):
        k = zz(d)
        DGU[k] = (factor * turned(N[k], AB[...])).reshape(NX, part, 2 * ff)

    def downs(d):
        k = zz(d)
        DDN[k] = (0.5 * factor * turned(G[k], H[...])).reshape(NX, part, ff)

    def partial(ch):
        ab = AB[span(ch)]
        inv = INV[span(ch)]
        total = jnp.zeros((rows, 128), F32)
        for k in range(NY * NC):
            v = gain[k] * lax.dot_general(
                ab,
                GU[k].reshape(wide, 2 * ff),
                (((1,), (1,)), ((), ())),
                preferred_element_type=F32,
            )
            V[k] = v
            total = total + lanes_summed(v * (T[k, span(ch)].astype(F32) * inv))
        inner = jnp.sum(total, axis=1, keepdims=True) / model
        for k in range(NY * NC):
            unit = T[k, span(ch)].astype(F32) * inv
            PP[k % NC, k // NC, span(ch)] = (inv * (V[k] - unit * inner)).astype(BF16)

    zs, ds, pc = {}, {}, {}

    def x_step1(i):
        k = zz(ORDER[i])
        SX1[i, 0] = DGU[k, xx(2), :, gate].astype(BF16)
        SX1[i, 1] = DGU[k, xx(2), :, up].astype(BF16)
        net.send("x1", SX1.at[i, 0], RX1.at[i, 0], ("x1", i), x=xx(1))
        net.send("x1", SX1.at[i, 1], RX1.at[i, 1], ("x1", i), x=xx(-1))

    def x_step2(i):
        k = zz(ORDER[i])
        net.arrived(("x1", i), SX1.at[i])
        SX2[i, 0, :, gate] = (DGU[k, xx(1), :, gate] + RX1[i, 0].astype(F32)).astype(BF16)
        SX2[i, 0, :, up] = DGU[k, xx(1), :, up].astype(BF16)
        net.send("x2", SX2.at[i, 0], RX2.at[i, 0], ("x2", i), x=xx(1))
        SX2[i, 1, :, gate] = DGU[k, xx(-1), :, gate].astype(BF16)
        SX2[i, 1, :, up] = (DGU[k, xx(-1), :, up] + RX1[i, 1].astype(F32)).astype(BF16)
        net.send("x2", SX2.at[i, 1], RX2.at[i, 1], ("x2", i), x=xx(-1))

    def x_sum(i):
        net.arrived(("x2", i), SX2.at[i])
        return DGU[zz(ORDER[i]), x] + RX2[i, 0].astype(F32) + RX2[i, 1].astype(F32)

    def z_step(i):
        d = ORDER[i]
        value = x_sum(i)
        if d == NZ // 2:
            SZ[0, 0] = value.astype(BF16)
            zs[1, d] = net.send("zs", SZ.at[0, 0, :, gate], RZ.at[0, 0, :, gate], z=zz(1))
            zs[-1, d] = net.send("zs", SZ.at[0, 0, :, up], RZ.at[0, 1, :, up], z=zz(-1))
            return None
        ways = (1, -1) if d == 0 else (1 if d > 0 else -1,)
        for way in ways:
            s, w = NZ // 2 - abs(d), 0 if way == 1 else 1
            zs[way, abs(d) + 1].wait_recv()
            if s == 1:
                cols = gate if way == 1 else up
                XR[...] = value
                XR[:, cols] = XR[:, cols] + RZ[0, w, :, cols].astype(F32)
                value = XR[...]
            else:
                value = value + RZ[s - 1, w].astype(F32)
            if d != 0:
                SZ[s, w] = value.astype(BF16)
                zs[way, abs(d)] = net.send("zs", SZ.at[s, w], RZ.at[s, w], z=zz(way))
        return value

    def d_step(d, way, half):
        k, w = zz(d), 0 if way == 1 else 1
        first = half == w
        blocks = pl.ds(half * (NX // 2), NX // 2)
        s = NZ // 2 - abs(d)
        value = DDN[k, blocks]
        if s >= (1 if first else 2):
            ds[way, half, abs(d) + 1].wait_recv()
            value = value + RD[s - 1, w, blocks].astype(F32)
        SD[s, w, blocks] = value.astype(BF16)
        group = "ds" if abs(d) == 1 else None
        ds[way, half, abs(d)] = net.send("ds",
            SD.at[s, w, blocks], RD.at[s, w, blocks], group, z=zz(way)
        )

    def d_both(s, old):
        for way in (1, -1):
            d_step(way * (NZ // 2 - s), way, (0 if way == 1 else 1) if old else (1 if way == 1 else 0))

    def d_sum():
        last = NZ // 2 - 1
        net.arrived("ds", SD.at[last])
        FD[...] = DDN[z] + RD[last, 0].astype(F32) + RD[last, 1].astype(F32)

    def e_step1():
        SE1[...] = FD[xx(2)].astype(BF16)
        lo, hi = pl.ds(0, half_part), pl.ds(half_part, half_part)
        net.send("e1", SE1.at[lo], RE1.at[lo], "e1", x=xx(1))
        net.send("e1", SE1.at[hi], RE1.at[hi], "e1", x=xx(-1))

    def e_step2():
        lo, hi = pl.ds(0, half_part), pl.ds(half_part, half_part)
        net.arrived("e1", SE1)
        SE2[0, lo] = (FD[xx(1), lo] + RE1[lo].astype(F32)).astype(BF16)
        SE2[0, hi] = FD[xx(1), hi].astype(BF16)
        net.send("e2", SE2.at[0], RE2.at[0], "e2", x=xx(1))
        SE2[1, lo] = FD[xx(-1), lo].astype(BF16)
        SE2[1, hi] = (FD[xx(-1), hi] + RE1[hi].astype(F32)).astype(BF16)
        net.send("e2", SE2.at[1], RE2.at[1], "e2", x=xx(-1))

    def e_sum():
        net.arrived("e2", SE2)
        return FD[x] + RE2[0].astype(F32) + RE2[1].astype(F32)

    def p_send(ch):
        pc[ch] = net.send("pc", PP.at[other, :, span(ch)], PR.at[:, span(ch)], c=other)

    def p_pair(ch, d, at, n):
        sub = pl.ds(ch * rows + at, n)
        return PP[c, yy(d), sub].astype(F32) + PR[yy(d), sub].astype(F32)

    def p_step1(ch):
        pc[ch].wait_recv()
        S1[ch] = p_pair(ch, 2, 0, rows).astype(BF16)
        lo, hi = pl.ds(0, half_rows), pl.ds(half_rows, half_rows)
        net.send("p1", S1.at[ch, lo], R1.at[ch, lo], ("p1", ch), y=yy(1))
        net.send("p1", S1.at[ch, hi], R1.at[ch, hi], ("p1", ch), y=yy(-1))

    def p_step2(ch):
        lo, hi = pl.ds(0, half_rows), pl.ds(half_rows, half_rows)
        net.arrived(("p1", ch), S1.at[ch])
        S2[ch, 0, lo] = (p_pair(ch, 1, 0, half_rows) + R1[ch, lo].astype(F32)).astype(BF16)
        S2[ch, 0, hi] = p_pair(ch, 1, half_rows, half_rows).astype(BF16)
        net.send("p2", S2.at[ch, 0], R2.at[ch, 0], ("p2", ch), y=yy(1))
        S2[ch, 1, lo] = p_pair(ch, -1, 0, half_rows).astype(BF16)
        S2[ch, 1, hi] = (
            p_pair(ch, -1, half_rows, half_rows) + R1[ch, hi].astype(F32)
        ).astype(BF16)
        net.send("p2", S2.at[ch, 1], R2.at[ch, 1], ("p2", ch), y=yy(-1))

    stores = []

    def store(src, dst):
        copy = pltpu.make_async_copy(src, dst, local_sems.at[len(loads) + len(stores)])
        copy.start()
        stores.append(copy)

    def p_sum(ch):
        net.arrived(("p2", ch), S2.at[ch])
        total = p_pair(ch, 0, 0, rows) + R2[ch, 0].astype(F32) + R2[ch, 1].astype(F32)
        IN[span(ch)] = (G[me, span(ch)].astype(F32) + total).astype(BF16)
        store(IN.at[span(ch)], out_in.at[span(ch)])

    def begin():
        locals_[0].wait()
        locals_[1].wait()
        y_own(0)
        for copy in locals_[2:5]:
            copy.wait()
        for way in (1, -1):
            gz[1, way] = net.send("gz", GU.at[z, x], GU.at[z, x], z=zz(way))
            dx[way] = net.send("dx", DN.at[z, x], DN.at[z, x], x=xx(way))
        dz_step(0, 0)
        gx_send(0, GU.at[z, x])
        for copy in locals_[5:]:
            copy.wait()
        y_own(1)
        net.send("c", T.at[me], T.at[me], ("c", 0), c=other)
        net.send("c", G.at[me], G.at[me], ("c", 0), c=other)

    def e_finish():
        down = e_sum()
        LD[...] = down
        store(LD, out_d)
        QA[z * NX + x, :, pl.ds(2 * ff, ff)] = jnp.sum(down * down, axis=0, keepdims=True)

    def z_finish():
        both = z_step(steps - 1)
        LG[...] = both[:, 0:ff]
        LU[...] = both[:, ff : 2 * ff]
        store(LG, out_g)
        store(LU, out_u)
        QA[z * NX + x, :, pl.ds(0, 2 * ff)] = jnp.sum(both * both, axis=0, keepdims=True)

    def q_all():
        for dz_ in (4, 3, 5, 2, 6, 1, 7, 0):
            for dx_ in (2, 1, 3, 0):
                if dz_ or dx_:
                    to = {}
                    if dz_:
                        to["z"] = zz(dz_)
                    if dx_:
                        to["x"] = xx(dx_)
                    net.send("q", QA.at[z * NX + x], QA.at[z * NX + x], "q", **to)
        for ch in range(CHUNKS):
            p_sum(ch)
        net.arrived("q", QA.at[pl.ds(0, NZ * NX - 1)])
        total = QA[0]
        for at in range(1, NZ * NX):
            total = total + QA[at]
        total = total / model
        for at in range(3):
            SQ[pl.ds(at, 1)] = total[:, at * ff : (at + 1) * ff]
        store(SQ, out_sq)

    def finish():
        assert net.used == ARRIVALS and len(net.kinds) == KINDS, net.used
        for kind, size in (
            ("gz", GU.at[pl.ds(0, NZ - 1), 0]),
            ("gx", GU.at[pl.ds(0, NZ // 2)]),
            ("gxf", DN.at[pl.ds(0, NZ // 2)]),
            ("dx", DN.at[0, pl.ds(0, 2)]),
            ("dxf", DN.at[0, 0]),
            ("dz", DN.at[pl.ds(0, NZ - 1)]),
            ("ya", PR),
            ("yb", PR.at[pl.ds(0, 2)]),
            ("c", PP),
            ("x1", SX1),
            ("x2", SX2),
            ("zs", SX2.at[pl.ds(0, NZ - 1), 0]),
            ("ds", DN.at[pl.ds(0, NZ - 1)]),
            ("e1", SE1),
            ("e2", SE2),
            ("pc", PR),
            ("p1", S1),
            ("p2", S2),
            ("q", QA.at[pl.ds(0, NZ * NX - 1)]),
        ):
            net.sent(kind, size)
        for copy in stores:
            copy.wait()

    steps = len(ORDER)
    begin()
    dx_pass()
    gz_step(1)
    dz_step(0, -1, 1)
    gx_pass(0)
    dz_step(1, 0)
    net.arrived("dxf", DN.at[0, 0])
    y_pass(0)
    y_own(2)
    gz_step(2)
    dz_step(0, 2)
    gx_pass(-1)
    dz_step(1, -1, 1)
    gx_pass(1)
    y_pass(1)
    y_own(3)
    y_own(4)
    gz_step(3)
    dz_step(2, 0)
    dz_step(1, 2)
    y_last(0)
    gx_pass(-2)
    gz_step(4)
    gx_pass(2)
    dz_step(2, -1, 1)
    dz_step(3, 0)
    dz_step(2, 2)
    y_pass(2)
    gx_pass(-3)
    gx_pass(3)
    dz_step(3, -1, 1)
    y_last(1)
    dz_step(3, 2)
    y_ready(0)
    norm(0)
    gx_pass(4)
    y_pass(3)
    y_ready(1)
    norm(1)
    net.arrived("dz", DN.at[0])
    net.arrived("gxf", DN.at[pl.ds(0, 4)])
    forward(0)
    y_pass(4)
    forward(1)
    y_last(2)
    y_ready(2)
    norm(2)
    y_last(3)
    forward(2)
    y_last(4)
    y_ready(3)
    norm(3)
    forward(3)
    y_ready(4)
    norm(4)
    forward(4)

    ahead = 4
    weights(ORDER[0])
    x_step1(0)
    weights(ORDER[1])
    x_step1(1)
    downs(ORDER[0])
    d_both(0, True)
    weights(ORDER[2])
    x_step1(2)
    downs(ORDER[1])
    downs(ORDER[2])
    d_both(1, False)
    weights(ORDER[3])
    x_step1(3)
    for i in range(5):
        x_step2(i)
        if i == 2:
            d_both(2, True)
        if i + ahead < steps:
            weights(ORDER[i + ahead])
            x_step1(i + ahead)
        if i == 0:
            downs(ORDER[3])
            downs(ORDER[4])
            d_both(1, True)
        if i == 1:
            d_both(2, False)
            downs(ORDER[5])
            downs(ORDER[6])
        if i == 3:
            d_both(3, True)
        if i >= 2:
            p_step1(i - 2)
        if i < CHUNKS:
            partial(i)
            p_send(i)
        if i == 2:
            d_both(3, False)
            downs(ORDER[7])
        if i >= 1:
            z_step(i - 1)
    x_step2(5)
    p_step1(3)
    p_step2(0)
    x_step2(6)
    p_step2(1)
    d_sum()
    e_step1()
    x_step2(7)
    z_step(4)
    p_step2(2)
    z_step(5)
    p_step2(3)
    z_step(6)
    e_step2()
    z_finish()
    e_finish()
    q_all()
    finish()


def deliver(*refs):
    n = (len(refs) - 2) // 3
    given, taken, held = refs[:n], refs[n : 2 * n], refs[2 * n : 3 * n]
    in_sems, out_sems = refs[3 * n :]
    parts = []
    for src, mid, dst in zip(given, held, taken):
        step = min(src.shape[0], 256)
        for at in range(0, src.shape[0], step):
            sub, i = pl.ds(at, step), len(parts)
            parts.append(
                (
                    pltpu.make_async_copy(src.at[sub], mid.at[sub], in_sems.at[i]),
                    pltpu.make_async_copy(mid.at[sub], dst.at[sub], out_sems.at[i]),
                )
            )
    for load, _ in parts:
        load.start()
    for load, save in parts:
        load.wait()
        save.start()
    for _, save in parts:
        save.wait()


def on_device(tokens, grad_out, norm_gain, gate_weight, up_weight, down_weight):
    n, wide = tokens.shape
    ff, part = gate_weight.shape
    blocks = NY * NC
    rows = n // CHUNKS
    gain = norm_gain.reshape(blocks, 1, wide)
    vm = pl.BlockSpec(memory_space=pltpu.VMEM)
    hbm = pl.BlockSpec(memory_space=pl.ANY)
    half = NZ // 2
    scratch = [
        ((blocks, n, wide), BF16),
        ((blocks, n, wide), BF16),
        ((blocks, n, wide), BF16),
        ((NZ, NX, part, 2 * ff), BF16),
        ((NZ, NX, part, ff), BF16),
        ((n, 2 * ff), BF16),
        ((n, ff), BF16),
        ((n, 1), F32),
        ((blocks, rows, wide), F32),
        ((NZ, NX, part, 2 * ff), F32),
        ((NZ, NX, part, ff), F32),
        ((NZ, 2, part, ff), BF16),
        ((NZ, 2, part, ff), BF16),
        ((NZ, 2, part, 2 * ff), BF16),
        ((NZ, 2, part, 2 * ff), BF16),
        ((part, 2 * ff), F32),
        ((half, 2, part, 2 * ff), BF16),
        ((half, 2, part, 2 * ff), BF16),
        ((half, 2, NX, part, ff), BF16),
        ((half, 2, NX, part, ff), BF16),
        ((NX, part, ff), F32),
        ((part, ff), BF16),
        ((part, ff), BF16),
        ((2, part, ff), BF16),
        ((2, part, ff), BF16),
        ((NC, NY, n, wide), BF16),
        ((NY, n, wide), BF16),
        ((CHUNKS, rows, wide), BF16),
        ((CHUNKS, rows, wide), BF16),
        ((CHUNKS, 2, rows, wide), BF16),
        ((CHUNKS, 2, rows, wide), BF16),
        ((NZ * NX, 1, 3 * ff), F32),
        ((n, wide), BF16),
        ((part, ff), F32),
        ((part, ff), F32),
        ((part, ff), F32),
        ((3, ff), F32),
    ]
    grad = jax.ShapeDtypeStruct((part, ff), F32)
    grad_in, grad_gate, grad_up, grad_down, squares = pl.pallas_call(
        kernel,
        out_shape=(
            jax.ShapeDtypeStruct((n, wide), BF16),
            grad,
            grad,
            grad,
            jax.ShapeDtypeStruct((3, ff), F32),
        ),
        in_specs=[hbm, hbm, vm, hbm, hbm, hbm],
        out_specs=(hbm,) * 5,
        scratch_shapes=[pltpu.VMEM(shape, dtype) for shape, dtype in scratch]
        + [
            pltpu.SemaphoreType.DMA((KINDS,)),
            pltpu.SemaphoreType.DMA((ARRIVALS,)),
            pltpu.SemaphoreType.DMA((15,)),
        ],
        compiler_params=pltpu.CompilerParams(
            collective_id=0, has_side_effects=True, vmem_limit_bytes=67043328
        ),
        name="ffn_backward",
    )(tokens, grad_out, gain, gate_weight.T, up_weight.T, down_weight.T)
    found = (grad_in, grad_gate, grad_up, grad_down, squares)
    results = pl.pallas_call(
        deliver,
        out_shape=tuple(jax.ShapeDtypeStruct(a.shape, a.dtype) for a in found),
        in_specs=[hbm] * 5,
        out_specs=(hbm,) * 5,
        scratch_shapes=[pltpu.VMEM(a.shape, a.dtype) for a in found]
        + [pltpu.SemaphoreType.DMA((8,)), pltpu.SemaphoreType.DMA((8,))],
        name="deliver",
    )(*found)
    grad_in, grad_gate, grad_up, grad_down, squares = results
    return grad_in, grad_gate.T, grad_up.T, grad_down.T, squares


def solution(mesh):
    split = Mesh(mesh.devices.reshape(NZ, NX, NY, NC), FS + TP)
    return jax.shard_map(
        on_device,
        mesh=split,
        in_specs=(P(FS, TP), P(FS, TP), P(), P(TP, FS), P(TP, FS), P(TP, FS)),
        out_specs=(P(FS, TP), P(TP, FS), P(TP, FS), P(TP, FS), P(None, TP)),
        check_vma=False,
    )
```

```python
import jax
import jax.numpy as jnp
from jax import lax
from jax.experimental import pallas as pl
from jax.experimental.pallas import tpu as pltpu
from jax.sharding import Mesh
from jax.sharding import PartitionSpec as P

FS = ("z", "x")
TP = ("y", "c")
NZ, NX, NY, NC = 8, 4, 4, 2
F32, BF16 = jnp.float32, jnp.bfloat16
CHUNKS = 4
ARRIVALS = 138
KINDS = 19
SPANS = ((0, 256), (256, 256), (512, 256), (768, 128), (896, 128))
ORDER = (4, 3, -3, 2, -2, 1, -1, 0)


class Net:
    def __init__(self, send_sems, recv_sems):
        self.send_sems, self.recv_sems = send_sems, recv_sems
        self.kinds, self.groups, self.used = [], {}, 0

    def send(self, kind, src, dst, group=None, **to):
        if kind not in self.kinds:
            self.kinds.append(kind)
        if group not in self.groups or group is None:
            self.groups[group] = self.used
            self.used += 1
        copy = pltpu.make_async_remote_copy(
            src_ref=src,
            dst_ref=dst,
            send_sem=self.send_sems.at[self.kinds.index(kind)],
            recv_sem=self.recv_sems.at[self.groups[group]],
            device_id=to,
            device_id_type=pl.DeviceIdType.MESH,
        )
        copy.start()
        return copy

    def arrived(self, group, size):
        pltpu.make_async_copy(size, size, self.recv_sems.at[self.groups[group]]).wait()

    def sent(self, kind, size):
        pltpu.make_async_copy(size, size, self.send_sems.at[self.kinds.index(kind)]).wait()


def lanes_summed(v):
    total = v[:, 0:128]
    for at in range(128, v.shape[1], 128):
        total = total + v[:, at : at + 128]
    return total


def turned(left, right):
    return lax.dot_general(left, right, (((0,), (0,)), ((), ())), preferred_element_type=F32)


def kernel(
    tok, grd, gains, wg, wu, wd,
    out_in, out_g, out_u, out_d, out_sq,
    T, G, N, GU, DN, AB, H, INV, V, DGU, DDN,
    SX1, RX1, SX2, RX2, XR, SZ, RZ, SD, RD, FD, SE1, RE1, SE2, RE2,
    PP, PR, S1, R1, S2, R2, QA, IN, LG, LU, LD, SQ, gain,
    send_sems, recv_sems, local_sems,
):
    z, x, y, c = (lax.axis_index(a) for a in ("z", "x", "y", "c"))
    zz = lambda d: lax.rem(z + (d + NZ), NZ)
    xx = lambda d: lax.rem(x + (d + NX), NX)
    yy = lambda d: lax.rem(y + (d + NY), NY)
    other = 1 - c
    me = y * NC + c
    slot = lambda d: yy(d) * NC + c
    tokens = tok.shape[0]
    rows = tokens // CHUNKS
    wide = tok.shape[1]
    part, ff = wd.shape
    model = wide * NY * NC
    half_part, half_rows = part // 2, rows // 2
    gate, up = pl.ds(0, ff), pl.ds(ff, ff)
    factor = (tokens * NZ * NX) ** (-0.5)
    span = lambda ch: pl.ds(ch * rows, rows)
    some = lambda ch: pl.ds(*SPANS[ch])

    barrier = pltpu.get_barrier_semaphore()
    peers = [{a: p} for a, n in (("z", zz), ("x", xx), ("y", yy)) for p in (n(1), n(-1))]
    peers += [{"c": other}]
    for peer in peers:
        pl.semaphore_signal(barrier, inc=1, device_id=peer, device_id_type=pl.DeviceIdType.MESH)
    head, rest = some(0), pl.ds(SPANS[0][1], tokens - SPANS[0][1])
    loads = (
        (tok.at[head], T.at[me, head]),
        (grd.at[head], G.at[me, head]),
        (wd, DN.at[z, x]),
        (wg, GU.at[z, x, :, gate]),
        (wu, GU.at[z, x, :, up]),
        (tok.at[rest], T.at[me, rest]),
        (grd.at[rest], G.at[me, rest]),
        (gains, gain),
    )
    locals_ = [
        pltpu.make_async_copy(src, dst, local_sems.at[i]) for i, (src, dst) in enumerate(loads)
    ]
    for copy in locals_:
        copy.start()
    pl.semaphore_wait(barrier, len(peers))
    net = Net(send_sems, recv_sems)

    gz, gx, dx, dz, ya, yb = {}, {}, {}, {}, {}, {}

    def gx_send(d, src):
        gx[d, 1] = net.send("gx", src, GU.at[zz(d), x], x=xx(1))
        gx[d, -1] = net.send("gx", src, GU.at[zz(d), x], x=xx(-1))

    def gx_pass(d):
        gx[d, 1].wait_recv()
        ref = GU.at[zz(d), xx(-1), :, gate]
        net.send("gxf", ref, ref, "gxf", x=xx(1))
        gx[d, -1].wait_recv()
        ref = GU.at[zz(d), xx(1), :, up]
        net.send("gxf", ref, ref, "gxf", x=xx(-1))

    def gz_step(s):
        for way in (1, -1):
            gz[s, way].wait_recv()
            if s < NZ // 2:
                ref = GU.at[zz(-way * s), x]
                if s == NZ // 2 - 1:
                    ref = GU.at[zz(-way * s), x, :, gate if way == 1 else up]
                gz[s + 1, way] = net.send("gz", ref, ref, z=zz(way))
        if s < NZ // 2:
            gx_send(-s, GU.at[zz(-s), x])
            gx_send(s, GU.at[zz(s), x])
        else:
            gx_send(s, GU.at[zz(s), x])

    def dx_pass():
        dx[1].wait_recv()
        ref = DN.at[z, xx(-1), pl.ds(0, half_part)]
        net.send("dxf", ref, ref, "dxf", x=xx(1))
        dx[-1].wait_recv()
        ref = DN.at[z, xx(1), pl.ds(half_part, half_part)]
        net.send("dxf", ref, ref, "dxf", x=xx(-1))

    def dz_step(s, *pieces):
        for dx_ in pieces:
            for way in (1, -1):
                if s > 0:
                    dz[s, dx_, way].wait_recv()
                ref = DN.at[zz(-way * s), xx(dx_)]
                if s < NZ // 2 - 1:
                    dz[s + 1, dx_, way] = net.send("dz", ref, ref, z=zz(way))
                elif (dx_ in (0, -1)) == (way == 1):
                    net.send("dz", ref, ref, "dz", z=zz(way))

    def y_own(ch):
        for way in (1, -1):
            ya["T", ch, way] = net.send("ya", T.at[me, some(ch)], T.at[me, some(ch)], y=yy(way))
            ya["G", ch, way] = net.send("ya", G.at[me, some(ch)], G.at[me, some(ch)], y=yy(way))

    def to_other(name, full, d, ch):
        ref = full.at[slot(d), some(ch)]
        net.send("c", ref, ref, ("c", ch), c=other)

    def y_pass(ch):
        ya["T", ch, 1].wait_recv()
        ref = T.at[slot(-1), some(ch)]
        yb["T", ch] = net.send("yb", ref, ref, y=yy(1))
        to_other("T", T, -1, ch)
        ya["G", ch, -1].wait_recv()
        ref = G.at[slot(1), some(ch)]
        yb["G", ch] = net.send("yb", ref, ref, y=yy(-1))
        to_other("G", G, 1, ch)
        ya["G", ch, 1].wait_recv()
        to_other("G", G, -1, ch)
        ya["T", ch, -1].wait_recv()
        to_other("T", T, 1, ch)

    def y_last(ch):
        yb["T", ch].wait_recv()
        to_other("T", T, 2, ch)
        yb["G", ch].wait_recv()
        to_other("G", G, 2, ch)

    def y_ready(ch):
        of_all = 6 * SPANS[ch][1] + (2 * tokens if ch == 0 else 0)
        lots = NY if ch == 0 else 3
        net.arrived(("c", ch), PP.at[0, pl.ds(0, lots), pl.ds(0, of_all // lots)])

    def norm(ch):
        total = jnp.zeros((SPANS[ch][1], 128), F32)
        for k in range(NY * NC):
            t = T[k, some(ch)].astype(F32)
            total = total + lanes_summed(t * t)
        inv = lax.rsqrt(jnp.sum(total, axis=1, keepdims=True) / model + 1e-06)
        INV[some(ch)] = inv
        for k in range(NY * NC):
            t = T[k, some(ch)].astype(F32)
            N[k, some(ch)] = (t * inv * gain[k]).astype(BF16)

    def forward(ch):
        pre = jnp.zeros((SPANS[ch][1], 2 * ff), F32)
        gh = jnp.zeros((SPANS[ch][1], ff), F32)
        for k in range(NY * NC):
            pre = pre + jnp.dot(
                N[k, some(ch)], GU[k].reshape(wide, 2 * ff), preferred_element_type=F32
            )
            gh = gh + jnp.dot(G[k, some(ch)], DN[k].reshape(wide, ff), preferred_element_type=F32)
        gh = 0.5 * gh
        g, u = pre[:, 0:ff], pre[:, ff : 2 * ff]
        sigma = jax.nn.sigmoid(g)
        active = g * sigma
        H[some(ch)] = (active * u).astype(BF16)
        AB[some(ch), 0:ff] = (gh * u * sigma * (1.0 + g * (1.0 - sigma))).astype(BF16)
        AB[some(ch), ff : 2 * ff] = (gh * active).astype(BF16)

    def weights(d):
        k = zz(d)
        DGU[k] = (factor * turned(N[k], AB[...])).reshape(NX, part, 2 * ff)

    def downs(d):
        k = zz(d)
        DDN[k] = (0.5 * factor * turned(G[k], H[...])).reshape(NX, part, ff)

    def partial(ch):
        ab = AB[span(ch)]
        inv = INV[span(ch)]
        total = jnp.zeros((rows, 128), F32)
        for k in range(NY * NC):
            v = gain[k] * lax.dot_general(
                ab,
                GU[k].reshape(wide, 2 * ff),
                (((1,), (1,)), ((), ())),
                preferred_element_type=F32,
            )
            V[k] = v
            total = total + lanes_summed(v * (T[k, span(ch)].astype(F32) * inv))
        inner = jnp.sum(total, axis=1, keepdims=True) / model
        for k in range(NY * NC):
            unit = T[k, span(ch)].astype(F32) * inv
            PP[k % NC, k // NC, span(ch)] = (inv * (V[k] - unit * inner)).astype(BF16)

    zs, ds, pc = {}, {}, {}

    def x_step1(i):
        k = zz(ORDER[i])
        SX1[i, 0] = DGU[k, xx(2), :, gate].astype(BF16)
        SX1[i, 1] = DGU[k, xx(2), :, up].astype(BF16)
        net.send("x1", SX1.at[i, 0], RX1.at[i, 0], ("x1", i), x=xx(1))
        net.send("x1", SX1.at[i, 1], RX1.at[i, 1], ("x1", i), x=xx(-1))

    def x_step2(i):
        k = zz(ORDER[i])
        net.arrived(("x1", i), SX1.at[i])
        SX2[i, 0, :, gate] = (DGU[k, xx(1), :, gate] + RX1[i, 0].astype(F32)).astype(BF16)
        SX2[i, 0, :, up] = DGU[k, xx(1), :, up].astype(BF16)
        net.send("x2", SX2.at[i, 0], RX2.at[i, 0], ("x2", i), x=xx(1))
        SX2[i, 1, :, gate] = DGU[k, xx(-1), :, gate].astype(BF16)
        SX2[i, 1, :, up] = (DGU[k, xx(-1), :, up] + RX1[i, 1].astype(F32)).astype(BF16)
        net.send("x2", SX2.at[i, 1], RX2.at[i, 1], ("x2", i), x=xx(-1))

    def x_sum(i):
        net.arrived(("x2", i), SX2.at[i])
        return DGU[zz(ORDER[i]), x] + RX2[i, 0].astype(F32) + RX2[i, 1].astype(F32)

    def z_step(i):
        d = ORDER[i]
        value = x_sum(i)
        if d == NZ // 2:
            SZ[0, 0] = value.astype(BF16)
            zs[1, d] = net.send("zs", SZ.at[0, 0, :, gate], RZ.at[0, 0, :, gate], z=zz(1))
            zs[-1, d] = net.send("zs", SZ.at[0, 0, :, up], RZ.at[0, 1, :, up], z=zz(-1))
            return None
        ways = (1, -1) if d == 0 else (1 if d > 0 else -1,)
        for way in ways:
            s, w = NZ // 2 - abs(d), 0 if way == 1 else 1
            zs[way, abs(d) + 1].wait_recv()
            if s == 1:
                cols = gate if way == 1 else up
                XR[...] = value
                XR[:, cols] = XR[:, cols] + RZ[0, w, :, cols].astype(F32)
                value = XR[...]
            else:
                value = value + RZ[s - 1, w].astype(F32)
            if d != 0:
                SZ[s, w] = value.astype(BF16)
                zs[way, abs(d)] = net.send("zs", SZ.at[s, w], RZ.at[s, w], z=zz(way))
        return value

    def d_step(d, way, half):
        k, w = zz(d), 0 if way == 1 else 1
        first = half == w
        blocks = pl.ds(half * (NX // 2), NX // 2)
        s = NZ // 2 - abs(d)
        value = DDN[k, blocks]
        if s >= (1 if first else 2):
            ds[way, half, abs(d) + 1].wait_recv()
            value = value + RD[s - 1, w, blocks].astype(F32)
        SD[s, w, blocks] = value.astype(BF16)
        group = "ds" if abs(d) == 1 else None
        ds[way, half, abs(d)] = net.send("ds",
            SD.at[s, w, blocks], RD.at[s, w, blocks], group, z=zz(way)
        )

    def d_both(s, old):
        for way in (1, -1):
            d_step(way * (NZ // 2 - s), way, (0 if way == 1 else 1) if old else (1 if way == 1 else 0))

    def d_sum():
        last = NZ // 2 - 1
        net.arrived("ds", SD.at[last])
        FD[...] = DDN[z] + RD[last, 0].astype(F32) + RD[last, 1].astype(F32)

    def e_step1():
        SE1[...] = FD[xx(2)].astype(BF16)
        lo, hi = pl.ds(0, half_part), pl.ds(half_part, half_part)
        net.send("e1", SE1.at[lo], RE1.at[lo], "e1", x=xx(1))
        net.send("e1", SE1.at[hi], RE1.at[hi], "e1", x=xx(-1))

    def e_step2():
        lo, hi = pl.ds(0, half_part), pl.ds(half_part, half_part)
        net.arrived("e1", SE1)
        SE2[0, lo] = (FD[xx(1), lo] + RE1[lo].astype(F32)).astype(BF16)
        SE2[0, hi] = FD[xx(1), hi].astype(BF16)
        net.send("e2", SE2.at[0], RE2.at[0], "e2", x=xx(1))
        SE2[1, lo] = FD[xx(-1), lo].astype(BF16)
        SE2[1, hi] = (FD[xx(-1), hi] + RE1[hi].astype(F32)).astype(BF16)
        net.send("e2", SE2.at[1], RE2.at[1], "e2", x=xx(-1))

    def e_sum():
        net.arrived("e2", SE2)
        return FD[x] + RE2[0].astype(F32) + RE2[1].astype(F32)

    def p_send(ch):
        pc[ch] = net.send("pc", PP.at[other, :, span(ch)], PR.at[:, span(ch)], c=other)

    def p_pair(ch, d, at, n):
        sub = pl.ds(ch * rows + at, n)
        return PP[c, yy(d), sub].astype(F32) + PR[yy(d), sub].astype(F32)

    def p_step1(ch):
        pc[ch].wait_recv()
        S1[ch] = p_pair(ch, 2, 0, rows).astype(BF16)
        lo, hi = pl.ds(0, half_rows), pl.ds(half_rows, half_rows)
        net.send("p1", S1.at[ch, lo], R1.at[ch, lo], ("p1", ch), y=yy(1))
        net.send("p1", S1.at[ch, hi], R1.at[ch, hi], ("p1", ch), y=yy(-1))

    def p_step2(ch):
        lo, hi = pl.ds(0, half_rows), pl.ds(half_rows, half_rows)
        net.arrived(("p1", ch), S1.at[ch])
        S2[ch, 0, lo] = (p_pair(ch, 1, 0, half_rows) + R1[ch, lo].astype(F32)).astype(BF16)
        S2[ch, 0, hi] = p_pair(ch, 1, half_rows, half_rows).astype(BF16)
        net.send("p2", S2.at[ch, 0], R2.at[ch, 0], ("p2", ch), y=yy(1))
        S2[ch, 1, lo] = p_pair(ch, -1, 0, half_rows).astype(BF16)
        S2[ch, 1, hi] = (
            p_pair(ch, -1, half_rows, half_rows) + R1[ch, hi].astype(F32)
        ).astype(BF16)
        net.send("p2", S2.at[ch, 1], R2.at[ch, 1], ("p2", ch), y=yy(-1))

    stores = []

    def store(src, dst):
        copy = pltpu.make_async_copy(src, dst, local_sems.at[len(loads) + len(stores)])
        copy.start()
        stores.append(copy)

    def p_sum(ch):
        net.arrived(("p2", ch), S2.at[ch])
        total = p_pair(ch, 0, 0, rows) + R2[ch, 0].astype(F32) + R2[ch, 1].astype(F32)
        IN[span(ch)] = (G[me, span(ch)].astype(F32) + total).astype(BF16)
        store(IN.at[span(ch)], out_in.at[span(ch)])

    def begin():
        locals_[0].wait()
        locals_[1].wait()
        y_own(0)
        for copy in locals_[2:5]:
            copy.wait()
        for way in (1, -1):
            gz[1, way] = net.send("gz", GU.at[z, x], GU.at[z, x], z=zz(way))
            dx[way] = net.send("dx", DN.at[z, x], DN.at[z, x], x=xx(way))
        dz_step(0, 0)
        gx_send(0, GU.at[z, x])
        for copy in locals_[5:]:
            copy.wait()
        y_own(1)
        net.send("c", T.at[me], T.at[me], ("c", 0), c=other)
        net.send("c", G.at[me], G.at[me], ("c", 0), c=other)

    def e_finish():
        down = e_sum()
        LD[...] = down
        store(LD, out_d)
        QA[z * NX + x, :, pl.ds(2 * ff, ff)] = jnp.sum(down * down, axis=0, keepdims=True)

    def z_finish():
        both = z_step(steps - 1)
        LG[...] = both[:, 0:ff]
        LU[...] = both[:, ff : 2 * ff]
        store(LG, out_g)
        store(LU, out_u)
        QA[z * NX + x, :, pl.ds(0, 2 * ff)] = jnp.sum(both * both, axis=0, keepdims=True)

    def q_all():
        for dz_ in (4, 3, 5, 2, 6, 1, 7, 0):
            for dx_ in (2, 1, 3, 0):
                if dz_ or dx_:
                    to = {}
                    if dz_:
                        to["z"] = zz(dz_)
                    if dx_:
                        to["x"] = xx(dx_)
                    net.send("q", QA.at[z * NX + x], QA.at[z * NX + x], "q", **to)
        for ch in range(CHUNKS):
            p_sum(ch)
        net.arrived("q", QA.at[pl.ds(0, NZ * NX - 1)])
        total = QA[0]
        for at in range(1, NZ * NX):
            total = total + QA[at]
        total = total / model
        for at in range(3):
            SQ[pl.ds(at, 1)] = total[:, at * ff : (at + 1) * ff]
        store(SQ, out_sq)

    def finish():
        assert net.used == ARRIVALS and len(net.kinds) == KINDS, net.used
        for kind, size in (
            ("gz", GU.at[pl.ds(0, NZ - 1), 0]),
            ("gx", GU.at[pl.ds(0, NZ // 2)]),
            ("gxf", DN.at[pl.ds(0, NZ // 2)]),
            ("dx", DN.at[0, pl.ds(0, 2)]),
            ("dxf", DN.at[0, 0]),
            ("dz", DN.at[pl.ds(0, NZ - 1)]),
            ("ya", PR),
            ("yb", PR.at[pl.ds(0, 2)]),
            ("c", PP),
            ("x1", SX1),
            ("x2", SX2),
            ("zs", SX2.at[pl.ds(0, NZ - 1), 0]),
            ("ds", DN.at[pl.ds(0, NZ - 1)]),
            ("e1", SE1),
            ("e2", SE2),
            ("pc", PR),
            ("p1", S1),
            ("p2", S2),
            ("q", QA.at[pl.ds(0, NZ * NX - 1)]),
        ):
            net.sent(kind, size)
        for copy in stores:
            copy.wait()

    steps = len(ORDER)
    begin()
    dx_pass()
    gz_step(1)
    dz_step(0, -1, 1)
    gx_pass(0)
    dz_step(1, 0)
    net.arrived("dxf", DN.at[0, 0])
    y_pass(0)
    y_own(2)
    gz_step(2)
    dz_step(0, 2)
    gx_pass(-1)
    dz_step(1, -1, 1)
    gx_pass(1)
    y_pass(1)
    y_own(3)
    y_own(4)
    gz_step(3)
    dz_step(2, 0)
    dz_step(1, 2)
    y_last(0)
    gx_pass(-2)
    gz_step(4)
    gx_pass(2)
    dz_step(2, -1, 1)
    dz_step(3, 0)
    dz_step(2, 2)
    y_pass(2)
    gx_pass(-3)
    gx_pass(3)
    dz_step(3, -1, 1)
    y_last(1)
    dz_step(3, 2)
    y_ready(0)
    norm(0)
    gx_pass(4)
    y_pass(3)
    y_ready(1)
    norm(1)
    net.arrived("dz", DN.at[0])
    net.arrived("gxf", DN.at[pl.ds(0, 4)])
    forward(0)
    y_pass(4)
    forward(1)
    y_last(2)
    y_ready(2)
    norm(2)
    y_last(3)
    forward(2)
    y_last(4)
    y_ready(3)
    norm(3)
    forward(3)
    y_ready(4)
    norm(4)
    forward(4)

    ahead = 4
    weights(ORDER[0])
    x_step1(0)
    weights(ORDER[1])
    x_step1(1)
    downs(ORDER[0])
    d_both(0, True)
    weights(ORDER[2])
    x_step1(2)
    weights(ORDER[3])
    x_step1(3)
    downs(ORDER[1])
    downs(ORDER[2])
    d_both(1, False)
    for i in range(5):
        x_step2(i)
        if i == 2:
            d_both(2, True)
        if i + ahead < steps:
            weights(ORDER[i + ahead])
            x_step1(i + ahead)
        if i == 0:
            downs(ORDER[3])
            downs(ORDER[4])
            d_both(1, True)
        if i == 1:
            d_both(2, False)
            downs(ORDER[5])
            downs(ORDER[6])
        if i == 3:
            d_both(3, True)
        if i >= 2:
            p_step1(i - 2)
        if i < CHUNKS:
            partial(i)
            p_send(i)
        if i == 2:
            d_both(3, False)
            downs(ORDER[7])
        if i >= 1:
            z_step(i - 1)
    x_step2(5)
    p_step1(3)
    p_step2(0)
    x_step2(6)
    p_step2(1)
    d_sum()
    e_step1()
    x_step2(7)
    z_step(4)
    p_step2(2)
    z_step(5)
    p_step2(3)
    z_step(6)
    e_step2()
    z_finish()
    e_finish()
    q_all()
    finish()


def deliver(*refs):
    n = (len(refs) - 2) // 3
    given, taken, held = refs[:n], refs[n : 2 * n], refs[2 * n : 3 * n]
    in_sems, out_sems = refs[3 * n :]
    parts = []
    for src, mid, dst in zip(given, held, taken):
        step = min(src.shape[0], 256)
        for at in range(0, src.shape[0], step):
            sub, i = pl.ds(at, step), len(parts)
            parts.append(
                (
                    pltpu.make_async_copy(src.at[sub], mid.at[sub], in_sems.at[i]),
                    pltpu.make_async_copy(mid.at[sub], dst.at[sub], out_sems.at[i]),
                )
            )
    for load, _ in parts:
        load.start()
    for load, save in parts:
        load.wait()
        save.start()
    for _, save in parts:
        save.wait()


def on_device(tokens, grad_out, norm_gain, gate_weight, up_weight, down_weight):
    n, wide = tokens.shape
    ff, part = gate_weight.shape
    blocks = NY * NC
    rows = n // CHUNKS
    gain = norm_gain.reshape(blocks, 1, wide)
    hbm = pl.BlockSpec(memory_space=pl.ANY)
    half = NZ // 2
    scratch = [
        ((blocks, n, wide), BF16),
        ((blocks, n, wide), BF16),
        ((blocks, n, wide), BF16),
        ((NZ, NX, part, 2 * ff), BF16),
        ((NZ, NX, part, ff), BF16),
        ((n, 2 * ff), BF16),
        ((n, ff), BF16),
        ((n, 1), F32),
        ((blocks, rows, wide), F32),
        ((NZ, NX, part, 2 * ff), F32),
        ((NZ, NX, part, ff), F32),
        ((NZ, 2, part, ff), BF16),
        ((NZ, 2, part, ff), BF16),
        ((NZ, 2, part, 2 * ff), BF16),
        ((NZ, 2, part, 2 * ff), BF16),
        ((part, 2 * ff), F32),
        ((half, 2, part, 2 * ff), BF16),
        ((half, 2, part, 2 * ff), BF16),
        ((half, 2, NX, part, ff), BF16),
        ((half, 2, NX, part, ff), BF16),
        ((NX, part, ff), F32),
        ((part, ff), BF16),
        ((part, ff), BF16),
        ((2, part, ff), BF16),
        ((2, part, ff), BF16),
        ((NC, NY, n, wide), BF16),
        ((NY, n, wide), BF16),
        ((CHUNKS, rows, wide), BF16),
        ((CHUNKS, rows, wide), BF16),
        ((CHUNKS, 2, rows, wide), BF16),
        ((CHUNKS, 2, rows, wide), BF16),
        ((NZ * NX, 1, 3 * ff), F32),
        ((n, wide), BF16),
        ((part, ff), F32),
        ((part, ff), F32),
        ((part, ff), F32),
        ((3, ff), F32),
        ((blocks, 1, wide), F32),
    ]
    grad = jax.ShapeDtypeStruct((part, ff), F32)
    grad_in, grad_gate, grad_up, grad_down, squares = pl.pallas_call(
        kernel,
        out_shape=(
            jax.ShapeDtypeStruct((n, wide), BF16),
            grad,
            grad,
            grad,
            jax.ShapeDtypeStruct((3, ff), F32),
        ),
        in_specs=[hbm] * 6,
        out_specs=(hbm,) * 5,
        scratch_shapes=[pltpu.VMEM(shape, dtype) for shape, dtype in scratch]
        + [
            pltpu.SemaphoreType.DMA((KINDS,)),
            pltpu.SemaphoreType.DMA((ARRIVALS,)),
            pltpu.SemaphoreType.DMA((16,)),
        ],
        compiler_params=pltpu.CompilerParams(
            collective_id=0, has_side_effects=True, vmem_limit_bytes=67043328
        ),
        name="ffn_backward",
    )(tokens, grad_out, gain, gate_weight.T, up_weight.T, down_weight.T)
    found = (grad_in, grad_gate, grad_up, grad_down, squares)
    results = pl.pallas_call(
        deliver,
        out_shape=tuple(jax.ShapeDtypeStruct(a.shape, a.dtype) for a in found),
        in_specs=[hbm] * 5,
        out_specs=(hbm,) * 5,
        scratch_shapes=[pltpu.VMEM(a.shape, a.dtype) for a in found]
        + [pltpu.SemaphoreType.DMA((8,)), pltpu.SemaphoreType.DMA((8,))],
        name="deliver",
    )(*found)
    grad_in, grad_gate, grad_up, grad_down, squares = results
    return grad_in, grad_gate.T, grad_up.T, grad_down.T, squares


def solution(mesh):
    split = Mesh(mesh.devices.reshape(NZ, NX, NY, NC), FS + TP)
    return jax.shard_map(
        on_device,
        mesh=split,
        in_specs=(P(FS, TP), P(FS, TP), P(), P(TP, FS), P(TP, FS), P(TP, FS)),
        out_specs=(P(FS, TP), P(TP, FS), P(TP, FS), P(TP, FS), P(None, TP)),
        check_vma=False,
    )
```

```python
import jax
import jax.numpy as jnp
from jax import lax
from jax.experimental import pallas as pl
from jax.experimental.pallas import tpu as pltpu
from jax.sharding import Mesh
from jax.sharding import PartitionSpec as P

FS = ("z", "x")
TP = ("y", "c")
NZ, NX, NY, NC = 8, 4, 4, 2
F32, BF16 = jnp.float32, jnp.bfloat16
CHUNKS = 4
ARRIVALS = 138
KINDS = 19
SPANS = ((0, 256), (256, 256), (512, 256), (768, 128), (896, 128))
ORDER = (4, 3, -3, 2, -2, 1, -1, 0)


class Net:
    def __init__(self, send_sems, recv_sems):
        self.send_sems, self.recv_sems = send_sems, recv_sems
        self.kinds, self.groups, self.used = [], {}, 0

    def send(self, kind, src, dst, group=None, **to):
        if kind not in self.kinds:
            self.kinds.append(kind)
        if group not in self.groups or group is None:
            self.groups[group] = self.used
            self.used += 1
        copy = pltpu.make_async_remote_copy(
            src_ref=src,
            dst_ref=dst,
            send_sem=self.send_sems.at[self.kinds.index(kind)],
            recv_sem=self.recv_sems.at[self.groups[group]],
            device_id=to,
            device_id_type=pl.DeviceIdType.MESH,
        )
        copy.start()
        return copy

    def arrived(self, group, size):
        pltpu.make_async_copy(size, size, self.recv_sems.at[self.groups[group]]).wait()

    def sent(self, kind, size):
        pltpu.make_async_copy(size, size, self.send_sems.at[self.kinds.index(kind)]).wait()


def lanes_summed(v):
    total = v[:, 0:128]
    for at in range(128, v.shape[1], 128):
        total = total + v[:, at : at + 128]
    return total


def turned(left, right):
    return lax.dot_general(left, right, (((0,), (0,)), ((), ())), preferred_element_type=F32)


def kernel(
    tok, grd, gains, wg, wu, wd,
    out_in, out_g, out_u, out_d, out_sq,
    T, G, N, GU, DN, AB, H, INV, V, DGU, DDN,
    SX1, RX1, SX2, RX2, XR, SZ, RZ, SD, RD, FD, SE1, RE1, SE2, RE2,
    PP, PR, S1, R1, S2, R2, QA, IN, LG, LU, LD, SQ, gain,
    send_sems, recv_sems, local_sems,
):
    z, x, y, c = (lax.axis_index(a) for a in ("z", "x", "y", "c"))
    zz = lambda d: lax.rem(z + (d + NZ), NZ)
    xx = lambda d: lax.rem(x + (d + NX), NX)
    yy = lambda d: lax.rem(y + (d + NY), NY)
    other = 1 - c
    me = y * NC + c
    slot = lambda d: yy(d) * NC + c
    tokens = tok.shape[0]
    rows = tokens // CHUNKS
    wide = tok.shape[1]
    part, ff = wd.shape
    model = wide * NY * NC
    half_part, half_rows = part // 2, rows // 2
    gate, up = pl.ds(0, ff), pl.ds(ff, ff)
    factor = (tokens * NZ * NX) ** (-0.5)
    span = lambda ch: pl.ds(ch * rows, rows)
    some = lambda ch: pl.ds(*SPANS[ch])

    barrier = pltpu.get_barrier_semaphore()
    peers = [{a: p} for a, n in (("z", zz), ("x", xx), ("y", yy)) for p in (n(1), n(-1))]
    peers += [{"c": other}]
    for peer in peers:
        pl.semaphore_signal(barrier, inc=1, device_id=peer, device_id_type=pl.DeviceIdType.MESH)
    head, rest = some(0), pl.ds(SPANS[0][1], tokens - SPANS[0][1])
    loads = (
        (tok.at[head], T.at[me, head]),
        (grd.at[head], G.at[me, head]),
        (wd, DN.at[z, x]),
        (wg, GU.at[z, x, :, gate]),
        (wu, GU.at[z, x, :, up]),
        (tok.at[rest], T.at[me, rest]),
        (grd.at[rest], G.at[me, rest]),
        (gains, gain),
    )
    locals_ = [
        pltpu.make_async_copy(src, dst, local_sems.at[i]) for i, (src, dst) in enumerate(loads)
    ]
    for copy in locals_:
        copy.start()
    pl.semaphore_wait(barrier, len(peers))
    net = Net(send_sems, recv_sems)

    gz, gx, dx, dz, ya, yb = {}, {}, {}, {}, {}, {}

    def gx_send(d, src):
        gx[d, 1] = net.send("gx", src, GU.at[zz(d), x], x=xx(1))
        gx[d, -1] = net.send("gx", src, GU.at[zz(d), x], x=xx(-1))

    def gx_pass(d):
        gx[d, 1].wait_recv()
        ref = GU.at[zz(d), xx(-1), :, gate]
        net.send("gxf", ref, ref, "gxf", x=xx(1))
        gx[d, -1].wait_recv()
        ref = GU.at[zz(d), xx(1), :, up]
        net.send("gxf", ref, ref, "gxf", x=xx(-1))

    def gz_step(s):
        for way in (1, -1):
            gz[s, way].wait_recv()
            if s < NZ // 2:
                ref = GU.at[zz(-way * s), x]
                if s == NZ // 2 - 1:
                    ref = GU.at[zz(-way * s), x, :, gate if way == 1 else up]
                gz[s + 1, way] = net.send("gz", ref, ref, z=zz(way))
        if s < NZ // 2:
            gx_send(-s, GU.at[zz(-s), x])
            gx_send(s, GU.at[zz(s), x])
        else:
            gx_send(s, GU.at[zz(s), x])

    def dx_pass():
        dx[1].wait_recv()
        ref = DN.at[z, xx(-1), pl.ds(0, half_part)]
        net.send("dxf", ref, ref, "dxf", x=xx(1))
        dx[-1].wait_recv()
        ref = DN.at[z, xx(1), pl.ds(half_part, half_part)]
        net.send("dxf", ref, ref, "dxf", x=xx(-1))

    def dz_step(s, *pieces):
        for dx_ in pieces:
            for way in (1, -1):
                if s > 0:
                    dz[s, dx_, way].wait_recv()
                ref = DN.at[zz(-way * s), xx(dx_)]
                if s < NZ // 2 - 1:
                    dz[s + 1, dx_, way] = net.send("dz", ref, ref, z=zz(way))
                elif (dx_ in (0, -1)) == (way == 1):
                    net.send("dz", ref, ref, "dz", z=zz(way))

    def y_own(ch):
        for way in (1, -1):
            ya["T", ch, way] = net.send("ya", T.at[me, some(ch)], T.at[me, some(ch)], y=yy(way))
            ya["G", ch, way] = net.send("ya", G.at[me, some(ch)], G.at[me, some(ch)], y=yy(way))

    def to_other(name, full, d, ch):
        ref = full.at[slot(d), some(ch)]
        net.send("c", ref, ref, ("c", ch), c=other)

    def y_pass(ch):
        ya["T", ch, 1].wait_recv()
        ref = T.at[slot(-1), some(ch)]
        yb["T", ch] = net.send("yb", ref, ref, y=yy(1))
        to_other("T", T, -1, ch)
        ya["G", ch, -1].wait_recv()
        ref = G.at[slot(1), some(ch)]
        yb["G", ch] = net.send("yb", ref, ref, y=yy(-1))
        to_other("G", G, 1, ch)
        ya["G", ch, 1].wait_recv()
        to_other("G", G, -1, ch)
        ya["T", ch, -1].wait_recv()
        to_other("T", T, 1, ch)

    def y_last(ch):
        yb["T", ch].wait_recv()
        to_other("T", T, 2, ch)
        yb["G", ch].wait_recv()
        to_other("G", G, 2, ch)

    def y_ready(ch):
        of_all = 6 * SPANS[ch][1] + (2 * tokens if ch == 0 else 0)
        lots = NY if ch == 0 else 3
        net.arrived(("c", ch), PP.at[0, pl.ds(0, lots), pl.ds(0, of_all // lots)])

    def norm(ch):
        total = jnp.zeros((SPANS[ch][1], 128), F32)
        for k in range(NY * NC):
            t = T[k, some(ch)].astype(F32)
            total = total + lanes_summed(t * t)
        inv = lax.rsqrt(jnp.sum(total, axis=1, keepdims=True) / model + 1e-06)
        INV[some(ch)] = inv
        for k in range(NY * NC):
            t = T[k, some(ch)].astype(F32)
            N[k, some(ch)] = (t * inv * gain[k]).astype(BF16)

    def forward(ch):
        pre = jnp.zeros((SPANS[ch][1], 2 * ff), F32)
        gh = jnp.zeros((SPANS[ch][1], ff), F32)
        for k in range(NY * NC):
            pre = pre + jnp.dot(
                N[k, some(ch)], GU[k].reshape(wide, 2 * ff), preferred_element_type=F32
            )
            gh = gh + jnp.dot(G[k, some(ch)], DN[k].reshape(wide, ff), preferred_element_type=F32)
        gh = 0.5 * gh
        g, u = pre[:, 0:ff], pre[:, ff : 2 * ff]
        sigma = jax.nn.sigmoid(g)
        active = g * sigma
        H[some(ch)] = (active * u).astype(BF16)
        AB[some(ch), 0:ff] = (gh * u * sigma * (1.0 + g * (1.0 - sigma))).astype(BF16)
        AB[some(ch), ff : 2 * ff] = (gh * active).astype(BF16)

    def weights(d):
        k = zz(d)
        DGU[k] = (factor * turned(N[k], AB[...])).reshape(NX, part, 2 * ff)

    def downs(d):
        k = zz(d)
        DDN[k] = (0.5 * factor * turned(G[k], H[...])).reshape(NX, part, ff)

    def partial(ch):
        ab = AB[span(ch)]
        inv = INV[span(ch)]
        total = jnp.zeros((rows, 128), F32)
        for k in range(NY * NC):
            v = gain[k] * lax.dot_general(
                ab,
                GU[k].reshape(wide, 2 * ff),
                (((1,), (1,)), ((), ())),
                preferred_element_type=F32,
            )
            V[k] = v
            total = total + lanes_summed(v * (T[k, span(ch)].astype(F32) * inv))
        inner = jnp.sum(total, axis=1, keepdims=True) / model
        for k in range(NY * NC):
            unit = T[k, span(ch)].astype(F32) * inv
            PP[k % NC, k // NC, span(ch)] = (inv * (V[k] - unit * inner)).astype(BF16)

    zs, ds, pc = {}, {}, {}

    def x_step1(i):
        k = zz(ORDER[i])
        SX1[i, 0] = DGU[k, xx(2), :, gate].astype(BF16)
        SX1[i, 1] = DGU[k, xx(2), :, up].astype(BF16)
        net.send("x1", SX1.at[i, 0], RX1.at[i, 0], ("x1", i), x=xx(1))
        net.send("x1", SX1.at[i, 1], RX1.at[i, 1], ("x1", i), x=xx(-1))

    def x_step2(i):
        k = zz(ORDER[i])
        net.arrived(("x1", i), SX1.at[i])
        SX2[i, 0, :, gate] = (DGU[k, xx(1), :, gate] + RX1[i, 0].astype(F32)).astype(BF16)
        SX2[i, 0, :, up] = DGU[k, xx(1), :, up].astype(BF16)
        net.send("x2", SX2.at[i, 0], RX2.at[i, 0], ("x2", i), x=xx(1))
        SX2[i, 1, :, gate] = DGU[k, xx(-1), :, gate].astype(BF16)
        SX2[i, 1, :, up] = (DGU[k, xx(-1), :, up] + RX1[i, 1].astype(F32)).astype(BF16)
        net.send("x2", SX2.at[i, 1], RX2.at[i, 1], ("x2", i), x=xx(-1))

    def x_sum(i):
        net.arrived(("x2", i), SX2.at[i])
        return DGU[zz(ORDER[i]), x] + RX2[i, 0].astype(F32) + RX2[i, 1].astype(F32)

    def z_step(i):
        d = ORDER[i]
        value = x_sum(i)
        if d == NZ // 2:
            SZ[0, 0] = value.astype(BF16)
            zs[1, d] = net.send("zs", SZ.at[0, 0, :, gate], RZ.at[0, 0, :, gate], z=zz(1))
            zs[-1, d] = net.send("zs", SZ.at[0, 0, :, up], RZ.at[0, 1, :, up], z=zz(-1))
            return None
        ways = (1, -1) if d == 0 else (1 if d > 0 else -1,)
        for way in ways:
            s, w = NZ // 2 - abs(d), 0 if way == 1 else 1
            zs[way, abs(d) + 1].wait_recv()
            if s == 1:
                cols = gate if way == 1 else up
                XR[...] = value
                XR[:, cols] = XR[:, cols] + RZ[0, w, :, cols].astype(F32)
                value = XR[...]
            else:
                value = value + RZ[s - 1, w].astype(F32)
            if d != 0:
                SZ[s, w] = value.astype(BF16)
                zs[way, abs(d)] = net.send("zs", SZ.at[s, w], RZ.at[s, w], z=zz(way))
        return value

    def d_step(d, way, half):
        k, w = zz(d), 0 if way == 1 else 1
        first = half == w
        blocks = pl.ds(half * (NX // 2), NX // 2)
        s = NZ // 2 - abs(d)
        value = DDN[k, blocks]
        if s >= (1 if first else 2):
            ds[way, half, abs(d) + 1].wait_recv()
            value = value + RD[s - 1, w, blocks].astype(F32)
        SD[s, w, blocks] = value.astype(BF16)
        group = "ds" if abs(d) == 1 else None
        ds[way, half, abs(d)] = net.send("ds",
            SD.at[s, w, blocks], RD.at[s, w, blocks], group, z=zz(way)
        )

    def d_both(s, old):
        for way in (1, -1):
            d_step(way * (NZ // 2 - s), way, (0 if way == 1 else 1) if old else (1 if way == 1 else 0))

    def d_sum():
        last = NZ // 2 - 1
        net.arrived("ds", SD.at[last])
        FD[...] = DDN[z] + RD[last, 0].astype(F32) + RD[last, 1].astype(F32)

    def e_step1():
        SE1[...] = FD[xx(2)].astype(BF16)
        lo, hi = pl.ds(0, half_part), pl.ds(half_part, half_part)
        net.send("e1", SE1.at[lo], RE1.at[lo], "e1", x=xx(1))
        net.send("e1", SE1.at[hi], RE1.at[hi], "e1", x=xx(-1))

    def e_step2():
        lo, hi = pl.ds(0, half_part), pl.ds(half_part, half_part)
        net.arrived("e1", SE1)
        SE2[0, lo] = (FD[xx(1), lo] + RE1[lo].astype(F32)).astype(BF16)
        SE2[0, hi] = FD[xx(1), hi].astype(BF16)
        net.send("e2", SE2.at[0], RE2.at[0], "e2", x=xx(1))
        SE2[1, lo] = FD[xx(-1), lo].astype(BF16)
        SE2[1, hi] = (FD[xx(-1), hi] + RE1[hi].astype(F32)).astype(BF16)
        net.send("e2", SE2.at[1], RE2.at[1], "e2", x=xx(-1))

    def e_sum():
        net.arrived("e2", SE2)
        return FD[x] + RE2[0].astype(F32) + RE2[1].astype(F32)

    def p_send(ch):
        pc[ch] = net.send("pc", PP.at[other, :, span(ch)], PR.at[:, span(ch)], c=other)

    def p_pair(ch, d, at, n):
        sub = pl.ds(ch * rows + at, n)
        return PP[c, yy(d), sub].astype(F32) + PR[yy(d), sub].astype(F32)

    def p_step1(ch):
        pc[ch].wait_recv()
        S1[ch] = p_pair(ch, 2, 0, rows).astype(BF16)
        lo, hi = pl.ds(0, half_rows), pl.ds(half_rows, half_rows)
        net.send("p1", S1.at[ch, lo], R1.at[ch, lo], ("p1", ch), y=yy(1))
        net.send("p1", S1.at[ch, hi], R1.at[ch, hi], ("p1", ch), y=yy(-1))

    def p_step2(ch):
        lo, hi = pl.ds(0, half_rows), pl.ds(half_rows, half_rows)
        net.arrived(("p1", ch), S1.at[ch])
        S2[ch, 0, lo] = (p_pair(ch, 1, 0, half_rows) + R1[ch, lo].astype(F32)).astype(BF16)
        S2[ch, 0, hi] = p_pair(ch, 1, half_rows, half_rows).astype(BF16)
        net.send("p2", S2.at[ch, 0], R2.at[ch, 0], ("p2", ch), y=yy(1))
        S2[ch, 1, lo] = p_pair(ch, -1, 0, half_rows).astype(BF16)
        S2[ch, 1, hi] = (
            p_pair(ch, -1, half_rows, half_rows) + R1[ch, hi].astype(F32)
        ).astype(BF16)
        net.send("p2", S2.at[ch, 1], R2.at[ch, 1], ("p2", ch), y=yy(-1))

    stores = []

    def store(src, dst):
        copy = pltpu.make_async_copy(src, dst, local_sems.at[len(loads) + len(stores)])
        copy.start()
        stores.append(copy)

    def p_sum(ch):
        net.arrived(("p2", ch), S2.at[ch])
        total = p_pair(ch, 0, 0, rows) + R2[ch, 0].astype(F32) + R2[ch, 1].astype(F32)
        IN[span(ch)] = (G[me, span(ch)].astype(F32) + total).astype(BF16)
        store(IN.at[span(ch)], out_in.at[span(ch)])

    def begin():
        locals_[0].wait()
        locals_[1].wait()
        y_own(0)
        for copy in locals_[2:5]:
            copy.wait()
        for way in (1, -1):
            gz[1, way] = net.send("gz", GU.at[z, x], GU.at[z, x], z=zz(way))
            dx[way] = net.send("dx", DN.at[z, x], DN.at[z, x], x=xx(way))
        dz_step(0, 0)
        gx_send(0, GU.at[z, x])
        for copy in locals_[5:]:
            copy.wait()
        y_own(1)
        net.send("c", T.at[me], T.at[me], ("c", 0), c=other)
        net.send("c", G.at[me], G.at[me], ("c", 0), c=other)

    def e_finish():
        down = e_sum()
        LD[...] = down
        store(LD, out_d)
        QA[z * NX + x, :, pl.ds(2 * ff, ff)] = jnp.sum(down * down, axis=0, keepdims=True)

    def z_finish():
        both = z_step(steps - 1)
        LG[...] = both[:, 0:ff]
        LU[...] = both[:, ff : 2 * ff]
        store(LG, out_g)
        store(LU, out_u)
        QA[z * NX + x, :, pl.ds(0, 2 * ff)] = jnp.sum(both * both, axis=0, keepdims=True)

    def q_all():
        for dz_ in (4, 3, 5, 2, 6, 1, 7, 0):
            for dx_ in (2, 1, 3, 0):
                if dz_ or dx_:
                    to = {}
                    if dz_:
                        to["z"] = zz(dz_)
                    if dx_:
                        to["x"] = xx(dx_)
                    net.send("q", QA.at[z * NX + x], QA.at[z * NX + x], "q", **to)
        for ch in range(CHUNKS):
            p_sum(ch)
        net.arrived("q", QA.at[pl.ds(0, NZ * NX - 1)])
        total = QA[0]
        for at in range(1, NZ * NX):
            total = total + QA[at]
        total = total / model
        for at in range(3):
            SQ[pl.ds(at, 1)] = total[:, at * ff : (at + 1) * ff]
        store(SQ, out_sq)

    def finish():
        assert net.used == ARRIVALS and len(net.kinds) == KINDS, net.used
        for kind, size in (
            ("gz", GU.at[pl.ds(0, NZ - 1), 0]),
            ("gx", GU.at[pl.ds(0, NZ // 2)]),
            ("gxf", DN.at[pl.ds(0, NZ // 2)]),
            ("dx", DN.at[0, pl.ds(0, 2)]),
            ("dxf", DN.at[0, 0]),
            ("dz", DN.at[pl.ds(0, NZ - 1)]),
            ("ya", PR),
            ("yb", PR.at[pl.ds(0, 2)]),
            ("c", PP),
            ("x1", SX1),
            ("x2", SX2),
            ("zs", SX2.at[pl.ds(0, NZ - 1), 0]),
            ("ds", DN.at[pl.ds(0, NZ - 1)]),
            ("e1", SE1),
            ("e2", SE2),
            ("pc", PR),
            ("p1", S1),
            ("p2", S2),
            ("q", QA.at[pl.ds(0, NZ * NX - 1)]),
        ):
            net.sent(kind, size)
        for copy in stores:
            copy.wait()

    steps = len(ORDER)
    begin()
    dx_pass()
    gz_step(1)
    dz_step(0, -1, 1)
    gx_pass(0)
    dz_step(1, 0)
    net.arrived("dxf", DN.at[0, 0])
    y_pass(0)
    y_own(2)
    gz_step(2)
    dz_step(0, 2)
    gx_pass(-1)
    dz_step(1, -1, 1)
    gx_pass(1)
    y_pass(1)
    y_own(3)
    y_own(4)
    gz_step(3)
    dz_step(2, 0)
    dz_step(1, 2)
    y_last(0)
    gx_pass(-2)
    gz_step(4)
    gx_pass(2)
    dz_step(2, -1, 1)
    dz_step(3, 0)
    dz_step(2, 2)
    y_pass(2)
    gx_pass(-3)
    gx_pass(3)
    dz_step(3, -1, 1)
    y_last(1)
    dz_step(3, 2)
    y_ready(0)
    norm(0)
    gx_pass(4)
    y_pass(3)
    y_ready(1)
    norm(1)
    net.arrived("dz", DN.at[0])
    net.arrived("gxf", DN.at[pl.ds(0, 4)])
    forward(0)
    y_pass(4)
    forward(1)
    y_last(2)
    y_ready(2)
    norm(2)
    y_last(3)
    forward(2)
    y_last(4)
    y_ready(3)
    norm(3)
    forward(3)
    y_ready(4)
    norm(4)
    forward(4)

    ahead = 4
    weights(ORDER[0])
    x_step1(0)
    weights(ORDER[1])
    x_step1(1)
    downs(ORDER[0])
    d_both(0, True)
    weights(ORDER[2])
    x_step1(2)
    weights(ORDER[3])
    x_step1(3)
    downs(ORDER[1])
    downs(ORDER[2])
    d_both(1, False)
    for i in range(5):
        x_step2(i)
        if i == 2:
            d_both(2, True)
        if i + ahead < steps:
            weights(ORDER[i + ahead])
            x_step1(i + ahead)
        if i == 0:
            downs(ORDER[3])
            downs(ORDER[4])
            d_both(1, True)
        if i == 1:
            d_both(2, False)
            downs(ORDER[5])
            downs(ORDER[6])
        if i == 3:
            d_both(3, True)
        if i >= 2:
            p_step1(i - 2)
        if i < CHUNKS:
            partial(i)
            p_send(i)
        if i == 2:
            d_both(3, False)
            downs(ORDER[7])
        if i >= 1:
            z_step(i - 1)
    x_step2(5)
    p_step1(3)
    p_step2(0)
    x_step2(6)
    p_step2(1)
    x_step2(7)
    d_sum()
    e_step1()
    z_step(4)
    p_step2(2)
    z_step(5)
    p_step2(3)
    z_step(6)
    e_step2()
    z_finish()
    e_finish()
    q_all()
    finish()


def deliver(*refs):
    n = (len(refs) - 2) // 3
    given, taken, held = refs[:n], refs[n : 2 * n], refs[2 * n : 3 * n]
    in_sems, out_sems = refs[3 * n :]
    parts = []
    for src, mid, dst in zip(given, held, taken):
        step = min(src.shape[0], 256)
        for at in range(0, src.shape[0], step):
            sub, i = pl.ds(at, step), len(parts)
            parts.append(
                (
                    pltpu.make_async_copy(src.at[sub], mid.at[sub], in_sems.at[i]),
                    pltpu.make_async_copy(mid.at[sub], dst.at[sub], out_sems.at[i]),
                )
            )
    for load, _ in parts:
        load.start()
    for load, save in parts:
        load.wait()
        save.start()
    for _, save in parts:
        save.wait()


def on_device(tokens, grad_out, norm_gain, gate_weight, up_weight, down_weight):
    n, wide = tokens.shape
    ff, part = gate_weight.shape
    blocks = NY * NC
    rows = n // CHUNKS
    gain = norm_gain.reshape(blocks, 1, wide)
    hbm = pl.BlockSpec(memory_space=pl.ANY)
    half = NZ // 2
    scratch = [
        ((blocks, n, wide), BF16),
        ((blocks, n, wide), BF16),
        ((blocks, n, wide), BF16),
        ((NZ, NX, part, 2 * ff), BF16),
        ((NZ, NX, part, ff), BF16),
        ((n, 2 * ff), BF16),
        ((n, ff), BF16),
        ((n, 1), F32),
        ((blocks, rows, wide), F32),
        ((NZ, NX, part, 2 * ff), F32),
        ((NZ, NX, part, ff), F32),
        ((NZ, 2, part, ff), BF16),
        ((NZ, 2, part, ff), BF16),
        ((NZ, 2, part, 2 * ff), BF16),
        ((NZ, 2, part, 2 * ff), BF16),
        ((part, 2 * ff), F32),
        ((half, 2, part, 2 * ff), BF16),
        ((half, 2, part, 2 * ff), BF16),
        ((half, 2, NX, part, ff), BF16),
        ((half, 2, NX, part, ff), BF16),
        ((NX, part, ff), F32),
        ((part, ff), BF16),
        ((part, ff), BF16),
        ((2, part, ff), BF16),
        ((2, part, ff), BF16),
        ((NC, NY, n, wide), BF16),
        ((NY, n, wide), BF16),
        ((CHUNKS, rows, wide), BF16),
        ((CHUNKS, rows, wide), BF16),
        ((CHUNKS, 2, rows, wide), BF16),
        ((CHUNKS, 2, rows, wide), BF16),
        ((NZ * NX, 1, 3 * ff), F32),
        ((n, wide), BF16),
        ((part, ff), F32),
        ((part, ff), F32),
        ((part, ff), F32),
        ((3, ff), F32),
        ((blocks, 1, wide), F32),
    ]
    grad = jax.ShapeDtypeStruct((part, ff), F32)
    grad_in, grad_gate, grad_up, grad_down, squares = pl.pallas_call(
        kernel,
        out_shape=(
            jax.ShapeDtypeStruct((n, wide), BF16),
            grad,
            grad,
            grad,
            jax.ShapeDtypeStruct((3, ff), F32),
        ),
        in_specs=[hbm] * 6,
        out_specs=(hbm,) * 5,
        scratch_shapes=[pltpu.VMEM(shape, dtype) for shape, dtype in scratch]
        + [
            pltpu.SemaphoreType.DMA((KINDS,)),
            pltpu.SemaphoreType.DMA((ARRIVALS,)),
            pltpu.SemaphoreType.DMA((16,)),
        ],
        compiler_params=pltpu.CompilerParams(
            collective_id=0, has_side_effects=True, vmem_limit_bytes=67043328
        ),
        name="ffn_backward",
    )(tokens, grad_out, gain, gate_weight.T, up_weight.T, down_weight.T)
    found = (grad_in, grad_gate, grad_up, grad_down, squares)
    results = pl.pallas_call(
        deliver,
        out_shape=tuple(jax.ShapeDtypeStruct(a.shape, a.dtype) for a in found),
        in_specs=[hbm] * 5,
        out_specs=(hbm,) * 5,
        scratch_shapes=[pltpu.VMEM(a.shape, a.dtype) for a in found]
        + [pltpu.SemaphoreType.DMA((8,)), pltpu.SemaphoreType.DMA((8,))],
        name="deliver",
    )(*found)
    grad_in, grad_gate, grad_up, grad_down, squares = results
    return grad_in, grad_gate.T, grad_up.T, grad_down.T, squares


def solution(mesh):
    split = Mesh(mesh.devices.reshape(NZ, NX, NY, NC), FS + TP)
    return jax.shard_map(
        on_device,
        mesh=split,
        in_specs=(P(FS, TP), P(FS, TP), P(), P(TP, FS), P(TP, FS), P(TP, FS)),
        out_specs=(P(FS, TP), P(TP, FS), P(TP, FS), P(TP, FS), P(None, TP)),
        check_vma=False,
    )
```
